256 devices in a mesh: sp: 128 (over z, y, x), tp: 2 (over core).
Axes of the slice: x: 4, y: 4, z: 8, core: 2. Of those that a mesh axis runs over, the one named last changes fastest.
Arguments:
- stream: bfloat16 [57344, 2048], P('sp'), may hold values from -6 to 6
- norm_gain: float32 [2, 2048], replicated, may hold values from 0.1 to 1.9
- value_weight: bfloat16 [2, 2048, 512], P(None, None, 'tp'), may hold values from -0.125 to 0.125
- gate_weight: bfloat16 [2, 2048, 512], P(None, None, 'tp'), may hold values from -0.125 to 0.125
- conv_taps: bfloat16 [2, 512, 512], P(None, None, 'tp'), may hold values from -0.25 to 0.25
- conv_bias: float32 [2, 512], P(None, 'tp'), may hold values from -3 to 3
- channel_gain: float32 [2, 512], replicated, may hold values from 0.1 to 1.9
- channel_shift: float32 [2, 512], replicated, may hold values from -3 to 3
- out_weight: bfloat16 [2, 512, 2048], replicated, may hold values from -0.25 to 0.25
Outputs:
- result: bfloat16 [57344, 2048], P('sp')
The draws below stay inside these ranges and needn't reach their ends.
All inputs are finite; a program needn't handle non-finite values.
Results may differ from the reference program's by a relative error of at most 0.0075.
Values may be sent and summed in bfloat16 or wider, within the bound.
A program may use at most 64 MiB of HBM per device.

```python
import jax
import jax.numpy as jnp
from jax import lax

D = 2048
CH = 512
KW = 512
LAYERS = 2
TOKENS = 57344


def block_scale(key, shape, pieces, smallest, high):
    loudness, own = 1.0, jax.random.fold_in(key, 6)
    for dim, parts in pieces:
        steps = jnp.exp(jax.random.uniform(jax.random.fold_in(own, dim), (parts,), jnp.float32, smallest / len(pieces), high / len(pieces)))
        loudness = loudness * jnp.repeat(steps, shape[dim] // parts).reshape([-1 if axis == dim else 1 for axis in range(len(shape))])
    return loudness


def scatter_about(stream_key, dims, scale, most, split=(), held_as=jnp.bfloat16):
    array = scale * jax.random.normal(stream_key, dims, jnp.float32)
    if split:
        array = array * block_scale(stream_key, dims, split, -0.22, 0.18)
    return jnp.clip(array, -most, most).astype(held_as)


def setup_inputs(seed: int = 0) -> dict:
    key_list = jax.random.split(jax.random.key(seed), 10)
    stream = scatter_about(key_list[0], (TOKENS, D), 1.0, 6.0, ((0, 128),))
    norm_gain = jnp.clip(1.0 + 0.18 * jax.random.normal(key_list[1], (LAYERS, D), jnp.float32), 0.1, 1.9)
    value_weight = scatter_about(key_list[2], (LAYERS, D, CH), D ** -0.5, 0.125, ((2, 2),))
    gate_weight = scatter_about(key_list[3], (LAYERS, D, CH), D ** -0.5, 0.125, ((2, 2),))
    conv_taps = scatter_about(key_list[4], (LAYERS, KW, CH), KW ** -0.5, 0.25, ((2, 2),))
    conv_bias = scatter_about(key_list[5], (LAYERS, CH), 0.5, 3.0, ((1, 2),), jnp.float32)
    channel_gain = jnp.clip(1.0 + 0.18 * jax.random.normal(key_list[6], (LAYERS, CH), jnp.float32), 0.1, 1.9)
    channel_shift = scatter_about(key_list[7], (LAYERS, CH), 0.5, 3.0, (), jnp.float32)
    out_weight = scatter_about(key_list[8], (LAYERS, CH, D), CH ** -0.5, 0.25)
    return dict(stream=stream, norm_gain=norm_gain, value_weight=value_weight, gate_weight=gate_weight, conv_taps=conv_taps, conv_bias=conv_bias, channel_gain=channel_gain, channel_shift=channel_shift, out_weight=out_weight)


def rms_normed(stream, gain):
    values = stream.astype(jnp.float32)
    scale = lax.rsqrt(lax.optimization_barrier(jnp.mean(values * values, axis=-1, keepdims=True)) + 1e-06)
    return (values * scale * gain[None, :]).astype(jnp.bfloat16)

def channel_mix(conv, gain, shift):
    values = conv.astype(jnp.float32)
    center = lax.optimization_barrier(jnp.mean(values, axis=-1, keepdims=True))
    spread = lax.optimization_barrier(jnp.mean(jnp.square(values - center), axis=-1, keepdims=True))
    normed = (values - center) * lax.rsqrt(spread + 1e-05) * gain[None, :] + shift[None, :]
    return jax.nn.silu(normed).astype(jnp.bfloat16)

def causal_conv(gated, taps):
    length = gated.shape[0]
    span = taps.shape[0]
    padded_len = 1 << (length + span - 2).bit_length()
    signal = jnp.fft.rfft(gated.astype(jnp.float32), n=padded_len, axis=0)
    kernel = jnp.fft.rfft(taps.astype(jnp.float32)[::-1], n=padded_len, axis=0)
    return jnp.fft.irfft(signal * kernel, n=padded_len, axis=0)[:length]

def reference(stream, norm_gain, value_weight, gate_weight, conv_taps, conv_bias, channel_gain, channel_shift, out_weight):
    state = stream
    for layer in range(LAYERS):
        normed = rms_normed(state, norm_gain[layer])
        values = jnp.dot(normed, value_weight[layer], preferred_element_type=jnp.float32)
        gates = jnp.dot(normed, gate_weight[layer], preferred_element_type=jnp.float32)
        gated = (values * jax.nn.sigmoid(gates)).astype(jnp.bfloat16)
        conv = causal_conv(gated, conv_taps[layer])
        conv = (conv + conv_bias[layer][None, :]).astype(jnp.bfloat16)
        mixed = channel_mix(conv, channel_gain[layer], channel_shift[layer])
        update = jnp.dot(mixed, out_weight[layer], preferred_element_type=jnp.float32)
        state = (state.astype(jnp.float32) + update).astype(jnp.bfloat16)
    return state
```

```python
import jax
import jax.numpy as jnp
import numpy as np
from jax import lax
from jax.sharding import PartitionSpec as P

BLOCK = 128
BF16 = jnp.bfloat16


def halves(matrix):
    high = matrix.astype(np.float32).astype(BF16)
    low = (matrix - high.astype(np.float64)).astype(np.float32).astype(BF16)
    return high, low


def spectra():
    odd = 2 * np.arange(BLOCK)[:, None] + 1
    n = np.arange(BLOCK)[None, :]
    angle = np.pi * odd * n / (2 * BLOCK)
    forward = np.concatenate([np.cos(angle), -np.sin(angle)])
    reverse = forward[:, ::-1]
    angle = angle + np.pi * odd / 2
    inverse = np.concatenate([np.cos(angle), -np.sin(angle)]).T / BLOCK
    return forward, reverse, inverse


def two_pass(matrix, blocks):
    high, low = halves(matrix)
    one = lambda m: jnp.einsum("fn,bnc->bfc", jnp.asarray(m), blocks, preferred_element_type=jnp.float32)
    return one(high) + one(low)


def causal_conv(window, taps):
    forward, reverse, inverse = spectra()
    channels = window.shape[1]
    signal = two_pass(forward, window.reshape(-1, BLOCK, channels))
    lags = two_pass(reverse, taps.reshape(-1, BLOCK, channels))[::-1]
    sign = jnp.asarray(np.where(np.arange(BLOCK) % 2, -1.0, 1.0).astype(np.float32))[None, :, None]
    re, im = lags[:, :BLOCK], lags[:, BLOCK:]
    turned_re, turned_im = sign * im, -sign * re
    zero = jnp.zeros_like(re[:1])
    h_re = jnp.concatenate([turned_re, zero]) + jnp.concatenate([zero, re])
    h_im = jnp.concatenate([turned_im, zero]) + jnp.concatenate([zero, im])
    a_re, a_im = signal[:, :BLOCK], signal[:, BLOCK:]
    count = signal.shape[0] - 4
    y_re = sum(h_re[c] * a_re[4 - c : 4 - c + count] - h_im[c] * a_im[4 - c : 4 - c + count] for c in range(5))
    y_im = sum(h_re[c] * a_im[4 - c : 4 - c + count] + h_im[c] * a_re[4 - c : 4 - c + count] for c in range(5))
    y = jnp.concatenate([y_re, y_im], axis=1)
    y_high = y.astype(BF16)
    y_low = (y - y_high.astype(jnp.float32)).astype(BF16)
    high, low = halves(inverse)
    one = lambda m, v: jnp.einsum("nf,bfc->bnc", jnp.asarray(m), v, preferred_element_type=jnp.float32)
    return (one(high, y_high) + one(high, y_low) + one(low, y_high)).reshape(-1, channels)


def passed_along(value, axis, by):
    count = lax.axis_size(axis)
    pairs = [(i, i + by) for i in range(count) if 0 <= i + by < count]
    return lax.ppermute(value, axis, pairs)


def rms_normed(stream, gain):
    values = stream.astype(jnp.float32)
    scale = lax.rsqrt(jnp.mean(values * values, axis=-1, keepdims=True) + 1e-06)
    return (values * scale * gain[None, :]).astype(jnp.bfloat16)


def channel_mix(conv, gain, shift):
    values = conv.astype(jnp.float32)
    center = jnp.mean(values, axis=-1, keepdims=True)
    spread = jnp.mean(jnp.square(values - center), axis=-1, keepdims=True)
    normed = (values - center) * lax.rsqrt(spread + 1e-05) * gain[None, :] + shift[None, :]
    return jax.nn.silu(normed).astype(jnp.bfloat16)


def gate_rows(normed, w_value, w_gate):
    values = jnp.dot(normed, w_value, preferred_element_type=jnp.float32)
    gates = jnp.dot(normed, w_gate, preferred_element_type=jnp.float32)
    return (values * jax.nn.sigmoid(gates)).astype(jnp.bfloat16)


def per_device(
    stream,
    norm_gain,
    value_weight,
    gate_weight,
    conv_taps,
    conv_bias,
    channel_gain,
    channel_shift,
    out_weight,
):
    tokens = stream.shape[0]
    reach = conv_taps.shape[1]
    hops = -(-reach // tokens)
    state = stream
    for layer in range(norm_gain.shape[0]):
        normed = rms_normed(state, norm_gain[layer])
        own_gated = gate_rows(normed, value_weight[layer], gate_weight[layer])
        pieces = [own_gated]
        for step in range(1, hops + 1):
            count = min(tokens, reach - (step - 1) * tokens)
            pieces.insert(0, passed_along(own_gated[tokens - count :], "sp", step))
        pieces.append(jnp.zeros((-(reach + tokens) % BLOCK, own_gated.shape[1]), own_gated.dtype))
        window = jnp.concatenate(pieces, axis=0)
        conv = causal_conv(window, conv_taps[layer])[:tokens]
        conv = (conv + conv_bias[layer][None, :]).astype(jnp.bfloat16)
        every_channel = lax.all_gather(conv, "tp", axis=1, tiled=True)
        mixed = channel_mix(every_channel, channel_gain[layer], channel_shift[layer])
        update = jnp.dot(mixed, out_weight[layer], preferred_element_type=jnp.float32)
        state = (state.astype(jnp.float32) + update).astype(jnp.bfloat16)
    return state


def solution(mesh):
    return jax.shard_map(
        per_device,
        mesh=mesh,
        in_specs=(
            P("sp", None),
            P(),
            P(None, None, "tp"),
            P(None, None, "tp"),
            P(None, None, "tp"),
            P(None, "tp"),
            P(),
            P(),
            P(),
        ),
        out_specs=P("sp", None),
        check_vma=False,
    )
```

```python
import functools

import jax
import jax.numpy as jnp
import numpy as np
from jax import lax
from jax.experimental import pallas as pl
from jax.experimental.pallas import tpu as pltpu
from jax.sharding import PartitionSpec as P

BLOCK = 128
CHUNK = 64
STRIP = 16
BF16 = jnp.bfloat16
F32 = jnp.float32
MESH = pl.DeviceIdType.MESH


def halves(matrix):
    high = matrix.astype(np.float32).astype(BF16)
    low = (matrix - high.astype(np.float64)).astype(np.float32).astype(BF16)
    return high, low


def spectra():
    odd = 2 * np.arange(BLOCK)[:, None] + 1
    angle = np.pi * odd * np.arange(BLOCK)[None, :] / (2 * BLOCK)
    forward = np.concatenate([np.cos(angle), -np.sin(angle)])
    reverse = forward[:, ::-1]
    angle = angle + np.pi * odd / 2
    inverse = np.concatenate([np.cos(angle), -np.sin(angle)]).T / BLOCK
    high, low = halves(inverse)
    return (
        np.concatenate(halves(forward), axis=1),
        np.concatenate(halves(reverse), axis=1),
        np.concatenate([high, high, low], axis=1),
    )


def kernel(
    devices,
    x_hbm, gain_hbm, wv_hbm, wg_hbm, taps_hbm, bias_hbm, cgain_hbm, cshift_hbm, wo_hbm, fwd_hbm, rev_hbm, inv_hbm,
    out_hbm,
    x, w, wo, taps, gain, bias, cgain, cshift, fwd, rev, inv,
    normed, own, halo, spec, lags, lag, prod, both, mixed, result,
    load_sem, send_sem, recv_sem, relay_send, relay_recv, pair_send, pair_recv, out_sem,
):
    tokens, width = x.shape
    layers = w.shape[0]
    half = w.shape[2] // 2
    chunks = tokens // CHUNK
    me, core = lax.axis_index("sp"), lax.axis_index("tp")
    after, before = lax.rem(me + 1, devices), lax.rem(me + devices - 1, devices)
    has_next, has_prev = me < devices - 1, me > 0

    barrier = pltpu.get_barrier_semaphore()
    pl.semaphore_signal(barrier, inc=1, device_id=(me, 1 - core), device_id_type=MESH)

    @pl.when(has_next)
    def _():
        pl.semaphore_signal(barrier, inc=1, device_id=(after, core), device_id_type=MESH)

    @pl.when(has_prev)
    def _():
        pl.semaphore_signal(barrier, inc=1, device_id=(before, core), device_id_type=MESH)

    loads = {}

    def load(name, source, target):
        loads[name] = pltpu.make_async_copy(source, target, load_sem.at[len(loads)])
        loads[name].start()

    def arrived(*names):
        for name in names:
            loads[name].wait()

    first = [(320, 448), (192, 320), (64, 192), (0, 64)]
    later = [(384, 448), (256, 384), (128, 256), (0, 128)]

    load("gain", gain_hbm, gain)
    load(("x", 0), x_hbm.at[pl.ds(320, 128)], x.at[pl.ds(320, 128)])
    load(("wv", 0), wv_hbm.at[0], w.at[0, :, pl.ds(0, half)])
    load(("wg", 0), wg_hbm.at[0], w.at[0, :, pl.ds(half, half)])
    for i in (1, 2, 3):
        rows = pl.ds(first[i][0], first[i][1] - first[i][0])
        load(("x", i), x_hbm.at[rows], x.at[rows])
    load("fwd", fwd_hbm, fwd)
    load("rev", rev_hbm, rev)
    load("taps", taps_hbm, taps)
    load("inv", inv_hbm, inv)
    load("bias", bias_hbm, bias)
    load("cgain", cgain_hbm, cgain)
    load("cshift", cshift_hbm, cshift)
    load(("wo", 0), wo_hbm.at[0], wo.at[0])
    load(("wv", 1), wv_hbm.at[1], w.at[1, :, pl.ds(0, half)])
    load(("wg", 1), wg_hbm.at[1], w.at[1, :, pl.ds(half, half)])
    load(("wo", 1), wo_hbm.at[1], wo.at[1])

    for layer in range(layers):
        own[layer, pl.ds(tokens, own.shape[1] - tokens), :] = jnp.zeros((own.shape[1] - tokens, half), BF16)

    @pl.when(me == 0)
    def _():
        halo[...] = jnp.zeros_like(halo)

    def chunk(layer, j):
        row = tokens - CHUNK * (j + 1)
        return pltpu.make_async_remote_copy(
            src_ref=own.at[layer, pl.ds(row, CHUNK)],
            dst_ref=halo.at[layer, pl.ds(CHUNK + row, CHUNK)],
            send_sem=send_sem.at[layer, j],
            recv_sem=recv_sem.at[layer, j],
            device_id=(after, core),
            device_id_type=MESH,
        )

    def relay(layer):
        return pltpu.make_async_remote_copy(
            src_ref=halo.at[layer, pl.ds(tokens, CHUNK)],
            dst_ref=halo.at[layer, pl.ds(0, CHUNK)],
            send_sem=relay_send.at[layer],
            recv_sem=relay_recv.at[layer],
            device_id=(after, core),
            device_id_type=MESH,
        )

    def pair(layer, m):
        low, high = later[3 - m]
        rows = pl.ds(low, high - low)
        return pltpu.make_async_remote_copy(
            src_ref=both.at[layer, core, rows],
            dst_ref=both.at[layer, core, rows],
            send_sem=pair_send.at[layer, m],
            recv_sem=pair_recv.at[layer, m],
            device_id=(me, 1 - core),
            device_id_type=MESH,
        )

    def strips(count, step):
        lax.fori_loop(0, count // STRIP, lambda i, c: (step(pl.multiple_of(i * STRIP, STRIP)), c)[1], 0, unroll=True)

    def project(layer, low, high):
        count = high - low

        def step(r):
            values = x[pl.ds(low + r, STRIP), :].astype(F32)
            scale = lax.rsqrt(jnp.sum(values * values, axis=-1, keepdims=True) * (1.0 / width) + 1e-06)
            normed[pl.ds(r, STRIP), :] = (values * scale * gain[pl.ds(layer, 1), :]).astype(BF16)

        strips(count, step)
        mm = jnp.dot(normed[pl.ds(0, count), :], w[layer], preferred_element_type=F32)
        own[layer, pl.ds(low, count), :] = (mm[:, :half] * jax.nn.sigmoid(mm[:, half:])).astype(BF16)

    def send(layer, low, high):
        @pl.when(has_next)
        def _():
            for j in range((tokens - high) // CHUNK, (tokens - low) // CHUNK):
                chunk(layer, j).start()

    def received(layer, *which):
        @pl.when(has_prev)
        def _():
            for j in which:
                if j < chunks:
                    chunk(layer, j).wait_recv()
                else:
                    relay(layer).wait_recv()

    def send_relay(layer):
        @pl.when(has_next)
        def _():
            relay(layer).start()

    def transform(layer, s):
        if s < 0:
            block = halo[layer, pl.ds(BLOCK * (s + 4), BLOCK), :]
        else:
            block = own[layer, pl.ds(BLOCK * s, BLOCK), :]
        spec[layer, s + 4] = jnp.dot(fwd[...], jnp.concatenate([block, block]), preferred_element_type=F32)

    def tap_spectra(layer):
        for b in range(4):
            block = taps[layer, pl.ds(BLOCK * (3 - b), BLOCK), :]
            lag[b] = jnp.dot(rev[...], jnp.concatenate([block, block]), preferred_element_type=F32)

        def step(i, carry):
            r = pl.multiple_of(i * STRIP, STRIP)
            odd = lax.rem(lax.broadcasted_iota(jnp.int32, (STRIP, half), 0), 2)
            sign = 1.0 - 2.0 * odd.astype(F32)
            re = [lag[b, pl.ds(r, STRIP), :] for b in range(4)]
            im = [lag[b, pl.ds(BLOCK + r, STRIP), :] for b in range(4)]
            for c in range(5):
                new_re, new_im = 0.0, 0.0
                if c < 4:
                    new_re, new_im = sign * im[c], -sign * re[c]
                if c > 0:
                    new_re, new_im = new_re + re[c - 1], new_im + im[c - 1]
                lags[layer, c, pl.ds(r, STRIP), :] = new_re
                lags[layer, c, pl.ds(BLOCK + r, STRIP), :] = new_im
            return carry

        lax.fori_loop(0, BLOCK // STRIP, step, 0, unroll=True)

    def convolve(layer, m):
        low, high = later[3 - m]

        def step(r):
            y_re, y_im = 0.0, 0.0
            for c in range(5):
                h_re, h_im = lags[layer, c, pl.ds(r, STRIP), :], lags[layer, c, pl.ds(BLOCK + r, STRIP), :]
                s = m - c + 4
                a_re, a_im = spec[layer, s, pl.ds(r, STRIP), :], spec[layer, s, pl.ds(BLOCK + r, STRIP), :]
                y_re = y_re + (h_re * a_re - h_im * a_im)
                y_im = y_im + (h_re * a_im + h_im * a_re)
            for at, y in ((0, y_re), (BLOCK, y_im)):
                top = y.astype(BF16)
                prod[pl.ds(at + r, STRIP), :] = top
                prod[pl.ds(2 * BLOCK + at + r, STRIP), :] = (y - top.astype(F32)).astype(BF16)
                prod[pl.ds(4 * BLOCK + at + r, STRIP), :] = top

        strips(BLOCK, step)
        conv = jnp.dot(inv[pl.ds(0, high - low), :], prod[...], preferred_element_type=F32)
        both[layer, core, pl.ds(low, high - low), :] = (conv + bias[pl.ds(layer, 1), :]).astype(BF16)
        pair(layer, m).start()

    def finish(layer, m):
        low, high = later[3 - m]
        count = high - low
        pair(layer, m).wait_recv()

        def step(r):
            parts = [both[layer, p, pl.ds(low + r, STRIP), :].astype(F32) for p in range(2)]
            center = sum(jnp.sum(v, axis=-1, keepdims=True) for v in parts) * (0.5 / half)
            parts = [v - center for v in parts]
            spread = sum(jnp.sum(v * v, axis=-1, keepdims=True) for v in parts) * (0.5 / half)
            scale = lax.rsqrt(spread + 1e-05)
            for p, v in enumerate(parts):
                columns = pl.ds(p * half, half)
                n = v * scale * cgain[pl.ds(layer, 1), columns] + cshift[pl.ds(layer, 1), columns]
                mixed[pl.ds(r, STRIP), columns] = (n * jax.nn.sigmoid(n)).astype(BF16)

        strips(count, step)
        rows = pl.ds(low, count)
        piece = 512
        target = x if layer < layers - 1 else result
        for at in range(0, width, piece):
            columns = pl.ds(at, piece)
            update = jnp.dot(mixed[pl.ds(0, count), :], wo[layer, :, columns], preferred_element_type=F32)
            target[rows, columns] = (x[rows, columns].astype(F32) + update).astype(BF16)

    def write(m):
        low, high = later[3 - m]
        rows = pl.ds(low, high - low)
        return pltpu.make_async_copy(result.at[rows], out_hbm.at[rows], out_sem.at[m])

    arrived("gain", ("x", 0))
    arrived(("wv", 0), ("wg", 0))
    project(0, *first[0])

    @pl.when(jnp.logical_and(has_prev, has_next))
    def _():
        pl.semaphore_wait(barrier, 3)

    @pl.when(jnp.logical_not(jnp.logical_and(has_prev, has_next)))
    def _():
        pl.semaphore_wait(barrier, 2)

    send(0, *first[0])
    for i in (1, 2, 3):
        arrived(("x", i))
        project(0, *first[i])
        send(0, *first[i])
    arrived("fwd", "rev", "taps", "inv", "bias", "cgain", "cshift")
    for s in (3, 2, 1, 0):
        transform(0, s)
    tap_spectra(0)
    tap_spectra(1)

    received(0, 0, 1)
    send_relay(0)
    transform(0, -1)
    convolve(0, 3)
    received(0, 2, 3)
    transform(0, -2)
    convolve(0, 2)
    arrived(("wo", 0), ("wv", 1), ("wg", 1))
    finish(0, 3)
    project(1, *later[0])
    send(1, *later[0])
    received(0, 4, 5)
    transform(0, -3)
    convolve(0, 1)
    finish(0, 2)
    project(1, *later[1])
    send(1, *later[1])
    received(0, 6, 7)
    transform(0, -4)
    convolve(0, 0)
    finish(0, 1)
    project(1, *later[2])
    send(1, *later[2])
    finish(0, 0)
    project(1, *later[3])
    send(1, *later[3])

    for s in (3, 2, 1, 0):
        transform(1, s)
    arrived(("wo", 1))
    received(1, 0, 1)
    send_relay(1)
    transform(1, -1)
    convolve(1, 3)
    received(1, 2, 3)
    transform(1, -2)
    convolve(1, 2)
    finish(1, 3)
    write(3).start()
    received(1, 4, 5)
    transform(1, -3)
    convolve(1, 1)
    finish(1, 2)
    write(2).start()
    received(1, 6, 7)
    transform(1, -4)
    convolve(1, 0)
    finish(1, 1)
    write(1).start()
    finish(1, 0)
    write(0).start()

    for layer in range(layers):
        for m in range(4):
            pair(layer, m).wait_send()

        @pl.when(has_next)
        def _():
            for j in range(chunks):
                chunk(layer, j).wait_send()
            relay(layer).wait_send()

    for m in range(4):
        write(m).wait()


def per_device(
    devices,
    stream,
    norm_gain,
    value_weight,
    gate_weight,
    conv_taps,
    conv_bias,
    channel_gain,
    channel_shift,
    out_weight,
):
    tokens, width = stream.shape
    layers, span, half = conv_taps.shape
    padded = -(-tokens // BLOCK) * BLOCK
    forward, reverse, inverse = (jnp.asarray(m) for m in spectra())
    dma = pltpu.SemaphoreType.DMA
    return pl.pallas_call(
        functools.partial(kernel, devices),
        out_shape=jax.ShapeDtypeStruct((tokens, width), BF16),
        in_specs=[pl.BlockSpec(memory_space=pl.ANY)] * 12,
        out_specs=pl.BlockSpec(memory_space=pl.ANY),
        scratch_shapes=[
            pltpu.VMEM((tokens, width), BF16),
            pltpu.VMEM((layers, width, 2 * half), BF16),
            pltpu.VMEM((layers, 2 * half, width), BF16),
            pltpu.VMEM((layers, span, half), BF16),
            pltpu.VMEM((layers, width), F32),
            pltpu.VMEM((layers, half), F32),
            pltpu.VMEM((layers, 2 * half), F32),
            pltpu.VMEM((layers, 2 * half), F32),
            pltpu.VMEM(forward.shape, BF16),
            pltpu.VMEM(reverse.shape, BF16),
            pltpu.VMEM(inverse.shape, BF16),
            pltpu.VMEM((BLOCK, width), BF16),
            pltpu.VMEM((layers, padded, half), BF16),
            pltpu.VMEM((layers, span, half), BF16),
            pltpu.VMEM((layers, 8, 2 * BLOCK, half), F32),
            pltpu.VMEM((layers, 5, 2 * BLOCK, half), F32),
            pltpu.VMEM((4, 2 * BLOCK, half), F32),
            pltpu.VMEM((6 * BLOCK, half), BF16),
            pltpu.VMEM((layers, 2, tokens, half), BF16),
            pltpu.VMEM((BLOCK, 2 * half), BF16),
            pltpu.VMEM((tokens, width), BF16),
            dma((24,)),
            dma((layers, tokens // CHUNK)),
            dma((layers, tokens // CHUNK)),
            dma((layers,)),
            dma((layers,)),
            dma((layers, 4)),
            dma((layers, 4)),
            dma((4,)),
        ],
        compiler_params=pltpu.CompilerParams(
            collective_id=0, has_side_effects=True, vmem_limit_bytes=60 * 1024 * 1024
        ),
        name="stacked_conv",
    )(
        stream, norm_gain, value_weight, gate_weight, conv_taps, conv_bias, channel_gain, channel_shift, out_weight,
        forward, reverse, inverse,
    )


def solution(mesh):
    return jax.shard_map(
        functools.partial(per_device, mesh.shape["sp"]),
        mesh=mesh,
        in_specs=(
            P("sp", None),
            P(),
            P(None, None, "tp"),
            P(None, None, "tp"),
            P(None, None, "tp"),
            P(None, "tp"),
            P(),
            P(),
            P(),
        ),
        out_specs=P("sp", None),
        check_vma=False,
    )
```

```python
import functools

import jax
import jax.numpy as jnp
import numpy as np
from jax import lax
from jax.experimental import pallas as pl
from jax.experimental.pallas import tpu as pltpu
from jax.sharding import PartitionSpec as P

BLOCK = 128
CHUNK = 64
STRIP = 16
BF16 = jnp.bfloat16
F32 = jnp.float32
LANES = 128
MESH = pl.DeviceIdType.MESH


def sigmoid(v):
    return 0.5 * jnp.tanh(0.5 * v) + 0.5


def halves(matrix):
    high = matrix.astype(np.float32).astype(BF16)
    low = (matrix - high.astype(np.float64)).astype(np.float32).astype(BF16)
    return high, low


def spectra():
    odd = 2 * np.arange(BLOCK)[:, None] + 1
    angle = np.pi * odd * np.arange(BLOCK)[None, :] / (2 * BLOCK)
    forward = np.concatenate([np.cos(angle), -np.sin(angle)])
    reverse = forward[:, ::-1]
    angle = angle + np.pi * odd / 2
    inverse = np.concatenate([np.cos(angle), -np.sin(angle)]).T / BLOCK
    high, low = halves(inverse)
    return (
        np.concatenate(halves(forward), axis=1),
        np.concatenate(halves(reverse), axis=1),
        np.concatenate([high, high, low], axis=1),
    )


def kernel(
    devices,
    x_hbm, gain_hbm, wv_hbm, wg_hbm, taps_hbm, bias_hbm, cgain_hbm, cshift_hbm, wo_hbm, fwd_hbm, rev_hbm, inv_hbm,
    out,
    x, w, wo, taps, gain, bias, cgain, cshift, fwd, rev, inv,
    normed, own, halo, spec, lags, lag, prod, part, scales, both, mixed,
    load_sem, send_sem, recv_sem, relay_send, relay_recv, pair_send, pair_recv,
):
    tokens, width = x.shape
    layers = w.shape[0]
    half = w.shape[2] // 2
    chunks = tokens // CHUNK
    me, core = lax.axis_index("sp"), lax.axis_index("tp")
    after, before = lax.rem(me + 1, devices), lax.rem(me + devices - 1, devices)
    has_next, has_prev = me < devices - 1, me > 0

    barrier = pltpu.get_barrier_semaphore()
    pl.semaphore_signal(barrier, inc=1, device_id=(me, 1 - core), device_id_type=MESH)

    @pl.when(has_prev)
    def _():
        pl.semaphore_signal(barrier, inc=1, device_id=(before, core), device_id_type=MESH)

    def scoped(f):
        def inner(*a):
            with jax.named_scope(f.__name__):
                return f(*a)

        return inner

    loads = {}

    def load(name, source, target):
        loads[name] = pltpu.make_async_copy(source, target, load_sem.at[len(loads)])
        loads[name].start()

    @scoped
    def arrived(*names):
        for name in names:
            loads[name].wait()

    first = [(320, 448), (192, 320), (64, 192), (0, 64)]
    later = [(384, 448), (256, 384), (128, 256), (0, 128)]

    load("gain", gain_hbm, gain)
    load(("x", 0), x_hbm.at[pl.ds(320, 128)], x.at[pl.ds(320, 128)])
    load(("wv", 0), wv_hbm.at[0], w.at[0, :, pl.ds(0, half)])
    load(("wg", 0), wg_hbm.at[0], w.at[0, :, pl.ds(half, half)])
    for i in (1, 2, 3):
        rows = pl.ds(first[i][0], first[i][1] - first[i][0])
        load(("x", i), x_hbm.at[rows], x.at[rows])
    load("fwd", fwd_hbm, fwd)
    load("rev", rev_hbm, rev)
    load("taps", taps_hbm, taps)
    load("inv", inv_hbm, inv)
    load("bias", bias_hbm, bias)
    load("cgain", cgain_hbm, cgain)
    load("cshift", cshift_hbm, cshift)
    load(("wo", 0), wo_hbm.at[0], wo.at[0])
    load(("wv", 1), wv_hbm.at[1], w.at[1, :, pl.ds(0, half)])
    load(("wg", 1), wg_hbm.at[1], w.at[1, :, pl.ds(half, half)])
    load(("wo", 1), wo_hbm.at[1], wo.at[1])

    for layer in range(layers):
        own[layer, pl.ds(tokens, own.shape[1] - tokens), :] = jnp.zeros((own.shape[1] - tokens, half), BF16)

    @pl.when(me == 0)
    def _():
        halo[...] = jnp.zeros_like(halo)

    def chunk(layer, j):
        row = tokens - CHUNK * (j + 1)
        return pltpu.make_async_remote_copy(
            src_ref=own.at[layer, pl.ds(row, CHUNK)],
            dst_ref=halo.at[layer, pl.ds(CHUNK + row, CHUNK)],
            send_sem=send_sem.at[layer, j],
            recv_sem=recv_sem.at[layer, j],
            device_id=(after, core),
            device_id_type=MESH,
        )

    def relay(layer):
        return pltpu.make_async_remote_copy(
            src_ref=halo.at[layer, pl.ds(tokens, CHUNK)],
            dst_ref=halo.at[layer, pl.ds(0, CHUNK)],
            send_sem=relay_send.at[layer],
            recv_sem=relay_recv.at[layer],
            device_id=(after, core),
            device_id_type=MESH,
        )

    def pair(layer, m):
        low, high = later[3 - m]
        rows = pl.ds(low, high - low)
        return pltpu.make_async_remote_copy(
            src_ref=both.at[layer, core, rows],
            dst_ref=both.at[layer, core, rows],
            send_sem=pair_send.at[layer, m],
            recv_sem=pair_recv.at[layer, m],
            device_id=(me, 1 - core),
            device_id_type=MESH,
        )

    def strips(count, step):
        lax.fori_loop(0, count // STRIP, lambda i, c: (step(pl.multiple_of(i * STRIP, STRIP)), c)[1], 0, unroll=True)

    def gate(layer, low, count, scale):
        mm = jnp.dot(normed[pl.ds(0, count), :], w[layer], preferred_element_type=F32)
        values, gates = mm[:, :half] * scale, mm[:, half:] * scale
        own[layer, pl.ds(low, count), :] = (values * sigmoid(gates)).astype(BF16)

    def row_scale(squares):
        return lax.rsqrt(jnp.sum(squares, axis=-1, keepdims=True) * (1.0 / width) + 1e-06)

    @scoped
    def prepare(low, high):
        count = high - low

        def step(r):
            values = x[pl.ds(low + r, STRIP), :].astype(F32)
            normed[pl.ds(r, STRIP), :] = (values * gain[pl.ds(0, 1), :]).astype(BF16)
            squares = sum(values[:, at : at + LANES] * values[:, at : at + LANES] for at in range(0, width, LANES))
            scales[pl.ds(r, STRIP), :] = jnp.broadcast_to(row_scale(squares), (STRIP, LANES))

        strips(count, step)

    @scoped
    def project(low, high):
        scale = scales[pl.ds(0, high - low), :]
        gate(0, low, high - low, jnp.concatenate([scale] * (half // LANES), axis=1))

    def send(layer, low, high):
        @pl.when(has_next)
        def _():
            for j in range((tokens - high) // CHUNK, (tokens - low) // CHUNK):
                chunk(layer, j).start()

    @scoped
    def received(layer, *which):
        @pl.when(has_prev)
        def _():
            for j in which:
                if j < chunks:
                    chunk(layer, j).wait_recv()
                else:
                    relay(layer).wait_recv()

    def send_relay(layer):
        @pl.when(has_next)
        def _():
            relay(layer).start()

    @scoped
    def transform(layer, s):
        if s < 0:
            block = halo[layer, pl.ds(BLOCK * (s + 4), BLOCK), :]
        else:
            block = own[layer, pl.ds(BLOCK * s, BLOCK), :]
        spec[layer, s + 4] = jnp.dot(fwd[...], jnp.concatenate([block, block]), preferred_element_type=F32)

    @scoped
    def tap_spectra(layer):
        for b in range(4):
            block = taps[layer, pl.ds(BLOCK * (3 - b), BLOCK), :]
            lag[b] = jnp.dot(rev[...], jnp.concatenate([block, block]), preferred_element_type=F32)

        def step(i, carry):
            r = pl.multiple_of(i * STRIP, STRIP)
            odd = lax.rem(lax.broadcasted_iota(jnp.int32, (STRIP, half), 0), 2)
            sign = 1.0 - 2.0 * odd.astype(F32)
            re = [lag[b, pl.ds(r, STRIP), :] for b in range(4)]
            im = [lag[b, pl.ds(BLOCK + r, STRIP), :] for b in range(4)]
            for c in range(5):
                new_re, new_im = 0.0, 0.0
                if c < 4:
                    new_re, new_im = sign * im[c], -sign * re[c]
                if c > 0:
                    new_re, new_im = new_re + re[c - 1], new_im + im[c - 1]
                lags[layer, c, pl.ds(r, STRIP), :] = new_re
                lags[layer, c, pl.ds(BLOCK + r, STRIP), :] = new_im
            return carry

        lax.fori_loop(0, BLOCK // STRIP, step, 0, unroll=True)

    def products(layer, m, r, taken):
        y_re, y_im = 0.0, 0.0
        for c in taken:
            h_re, h_im = lags[layer, c, pl.ds(r, STRIP), :], lags[layer, c, pl.ds(BLOCK + r, STRIP), :]
            s = m - c + 4
            a_re, a_im = spec[layer, s, pl.ds(r, STRIP), :], spec[layer, s, pl.ds(BLOCK + r, STRIP), :]
            y_re = y_re + (h_re * a_re - h_im * a_im)
            y_im = y_im + (h_re * a_im + h_im * a_re)
        return y_re, y_im

    @scoped
    def own_part(layer, since):
        for m in range(since, 4):

            def step(r):
                y_re, y_im = products(layer, m, r, range(m + 1 - since))
                part[m, pl.ds(r, STRIP), :] = y_re
                part[m, pl.ds(BLOCK + r, STRIP), :] = y_im

            strips(BLOCK, step)

    @scoped
    def convolve(layer, m, since):
        low, high = later[3 - m]

        def step(r):
            y_re, y_im = products(layer, m, r, range(max(m + 1 - since, 0), 5))
            if m >= since:
                y_re, y_im = y_re + part[m, pl.ds(r, STRIP), :], y_im + part[m, pl.ds(BLOCK + r, STRIP), :]
            for at, y in ((0, y_re), (BLOCK, y_im)):
                top = y.astype(BF16)
                prod[pl.ds(at + r, STRIP), :] = top
                prod[pl.ds(2 * BLOCK + at + r, STRIP), :] = (y - top.astype(F32)).astype(BF16)

        strips(BLOCK, step)
        rows = pl.ds(0, high - low)
        conv = jnp.dot(inv[rows, pl.ds(0, 4 * BLOCK)], prod[...], preferred_element_type=F32)
        conv += jnp.dot(inv[rows, pl.ds(4 * BLOCK, 2 * BLOCK)], prod[pl.ds(0, 2 * BLOCK), :], preferred_element_type=F32)
        both[layer, core, pl.ds(low, high - low), :] = (conv + bias[pl.ds(layer, 1), :]).astype(BF16)
        pair(layer, m).start()

    @scoped
    def paired(layer, *which):
        for m in which:
            pair(layer, m).wait_recv()

    @scoped
    def mix(layer, m):
        low, high = later[3 - m]

        def step(r):
            rows = pl.ds(low + r, STRIP)
            parts = [both[layer, p, rows, :].astype(F32) for p in range(2)]
            center = jnp.sum(parts[0] + parts[1], axis=-1, keepdims=True) * (0.5 / half)
            parts = [v - center for v in parts]
            spread = jnp.sum(parts[0] * parts[0] + parts[1] * parts[1], axis=-1, keepdims=True) * (0.5 / half)
            scale = lax.rsqrt(spread + 1e-05)
            for p, v in enumerate(parts):
                columns = pl.ds(p * half, half)
                n = v * scale * cgain[pl.ds(layer, 1), columns] + cshift[pl.ds(layer, 1), columns]
                mixed[rows, columns] = (n * sigmoid(n)).astype(BF16)

        strips(high - low, step)

    @scoped
    def finish(layer, *which):
        low, high = min(later[3 - m][0] for m in which), max(later[3 - m][1] for m in which)
        count = high - low
        rows = pl.ds(low, count)
        piece = 512
        squares = 0.0
        for at in range(0, width, piece):
            columns = pl.ds(at, piece)
            update = jnp.dot(mixed[rows, :], wo[layer, :, columns], preferred_element_type=F32)
            state = (x[rows, columns].astype(F32) + update).astype(BF16)
            if layer == layers - 1:
                out[rows, columns] = state
                continue
            x[rows, columns] = state
            state = state.astype(F32)
            normed[pl.ds(0, count), columns] = (state * gain[pl.ds(layer + 1, 1), columns]).astype(BF16)
            squares = squares + sum(state[:, q : q + LANES] * state[:, q : q + LANES] for q in range(0, piece, LANES))
        if layer < layers - 1:
            gate(layer + 1, low, count, row_scale(squares))
            send(layer + 1, low, high)

    arrived("gain", ("x", 0))
    prepare(*first[0])
    arrived(("wv", 0), ("wg", 0))
    project(*first[0])
    with jax.named_scope("barrier"):

        @pl.when(has_next)
        def _():
            pl.semaphore_wait(barrier, 2)

        @pl.when(jnp.logical_not(has_next))
        def _():
            pl.semaphore_wait(barrier, 1)

    send(0, *first[0])
    for i in (1, 2, 3):
        arrived(("x", i))
        prepare(*first[i])
        project(*first[i])
        send(0, *first[i])
    arrived("fwd", "rev", "taps", "inv", "bias", "cgain", "cshift")
    for s in (3, 2, 1, 0):
        transform(0, s)
    tap_spectra(0)
    own_part(0, 0)
    tap_spectra(1)

    for layer, since in ((0, 0), (1, 1)):
        received(layer, 0, 1)
        send_relay(layer)
        transform(layer, -1)
        convolve(layer, 3, since)
        received(layer, 2, 3)
        transform(layer, -2)
        convolve(layer, 2, since)
        if layer == 0:
            arrived(("wo", 0), ("wv", 1), ("wg", 1))
        received(layer, 4, 5)
        paired(layer, 3, 2)
        transform(layer, -3)
        convolve(layer, 1, since)
        mix(layer, 3)
        mix(layer, 2)
        finish(layer, 3, 2)
        received(layer, 6, 7)
        transform(layer, -4)
        convolve(layer, 0, since)
        paired(layer, 1)
        mix(layer, 1)
        finish(layer, 1)
        paired(layer, 0)
        mix(layer, 0)
        finish(layer, 0)
        if layer == 0:
            for s in (3, 2, 1, 0):
                transform(1, s)
            own_part(1, 1)
            arrived(("wo", 1))

    for layer in range(layers):
        for m in range(4):
            pair(layer, m).wait_send()

        @pl.when(has_next)
        def _():
            for j in range(chunks):
                chunk(layer, j).wait_send()
            relay(layer).wait_send()


def per_device(
    devices,
    stream,
    norm_gain,
    value_weight,
    gate_weight,
    conv_taps,
    conv_bias,
    channel_gain,
    channel_shift,
    out_weight,
):
    tokens, width = stream.shape
    layers, span, half = conv_taps.shape
    padded = -(-tokens // BLOCK) * BLOCK
    forward, reverse, inverse = (jnp.asarray(m) for m in spectra())
    dma = pltpu.SemaphoreType.DMA
    return pl.pallas_call(
        functools.partial(kernel, devices),
        out_shape=pltpu.VMEM((tokens, width), BF16),
        in_specs=[pl.BlockSpec(memory_space=pltpu.HBM)] * 12,
        out_specs=pl.BlockSpec(memory_space=pltpu.VMEM),
        scratch_shapes=[
            pltpu.VMEM((tokens, width), BF16),
            pltpu.VMEM((layers, width, 2 * half), BF16),
            pltpu.VMEM((layers, 2 * half, width), BF16),
            pltpu.VMEM((layers, span, half), BF16),
            pltpu.VMEM((layers, width), F32),
            pltpu.VMEM((layers, half), F32),
            pltpu.VMEM((layers, 2 * half), F32),
            pltpu.VMEM((layers, 2 * half), F32),
            pltpu.VMEM(forward.shape, BF16),
            pltpu.VMEM(reverse.shape, BF16),
            pltpu.VMEM(inverse.shape, BF16),
            pltpu.VMEM((2 * BLOCK, width), BF16),
            pltpu.VMEM((layers, padded, half), BF16),
            pltpu.VMEM((layers, span, half), BF16),
            pltpu.VMEM((layers, 8, 2 * BLOCK, half), F32),
            pltpu.VMEM((layers, 5, 2 * BLOCK, half), F32),
            pltpu.VMEM((4, 2 * BLOCK, half), F32),
            pltpu.VMEM((4 * BLOCK, half), BF16),
            pltpu.VMEM((4, 2 * BLOCK, half), F32),
            pltpu.VMEM((BLOCK, LANES), F32),
            pltpu.VMEM((layers, 2, tokens, half), BF16),
            pltpu.VMEM((tokens, 2 * half), BF16),
            dma((24,)),
            dma((layers, tokens // CHUNK)),
            dma((layers, tokens // CHUNK)),
            dma((layers,)),
            dma((layers,)),
            dma((layers, 4)),
            dma((layers, 4)),
        ],
        compiler_params=pltpu.CompilerParams(
            collective_id=0, has_side_effects=True, vmem_limit_bytes=60 * 1024 * 1024
        ),
        name="stacked_conv",
    )(
        stream, norm_gain, value_weight, gate_weight, conv_taps, conv_bias, channel_gain, channel_shift, out_weight,
        forward, reverse, inverse,
    )


def solution(mesh):
    return jax.shard_map(
        functools.partial(per_device, mesh.shape["sp"]),
        mesh=mesh,
        in_specs=(
            P("sp", None),
            P(),
            P(None, None, "tp"),
            P(None, None, "tp"),
            P(None, None, "tp"),
            P(None, "tp"),
            P(),
            P(),
            P(),
        ),
        out_specs=P("sp", None),
        check_vma=False,
    )
```

```python
import functools

import jax
import jax.numpy as jnp
import numpy as np
from jax import lax
from jax.experimental import pallas as pl
from jax.experimental.pallas import tpu as pltpu
from jax.sharding import PartitionSpec as P

BLOCK = 128
CHUNK = 64
STRIP = 16
BF16 = jnp.bfloat16
F32 = jnp.float32
LANES = 128
PIECES = 4
MESH = pl.DeviceIdType.MESH


def sigmoid(v):
    return 0.5 * jnp.tanh(0.5 * v) + 0.5


def halves(matrix):
    high = matrix.astype(np.float32).astype(BF16)
    low = (matrix - high.astype(np.float64)).astype(np.float32).astype(BF16)
    return high, low


def spectra():
    odd = 2 * np.arange(BLOCK)[:, None] + 1
    angle = np.pi * odd * np.arange(BLOCK)[None, :] / (2 * BLOCK)
    forward = np.concatenate([np.cos(angle), -np.sin(angle)])
    reverse = forward[:, ::-1]
    angle = angle + np.pi * odd / 2
    inverse = np.concatenate([np.cos(angle), -np.sin(angle)]).T / BLOCK
    high, low = halves(inverse)
    return (
        np.concatenate(halves(forward), axis=1),
        np.concatenate(halves(reverse), axis=1),
        np.concatenate([high, high, low], axis=1),
    )


def kernel(
    devices,
    x_hbm, gain_hbm, wv_hbm, wg_hbm, taps_hbm, bias_hbm, cgain_hbm, cshift_hbm, wo_hbm, fwd_hbm, rev_hbm, inv_hbm,
    out,
    x, w, wo, taps, gain, bias, cgain, cshift, fwd, rev, inv,
    normed, own, halo, spec, lags, lag, prod, part, scales, both, mixed,
    load_sem, send_sem, recv_sem, relay_send, relay_recv, pair_send, pair_recv,
):
    tokens, width = x.shape
    layers = w.shape[0]
    half = w.shape[2] // 2
    chunks = tokens // CHUNK
    me, core = lax.axis_index("sp"), lax.axis_index("tp")
    after, before = lax.rem(me + 1, devices), lax.rem(me + devices - 1, devices)
    has_next, has_prev = me < devices - 1, me > 0

    barrier = pltpu.get_barrier_semaphore()
    pl.semaphore_signal(barrier, inc=1, device_id=(me, 1 - core), device_id_type=MESH)

    @pl.when(has_prev)
    def _():
        pl.semaphore_signal(barrier, inc=1, device_id=(before, core), device_id_type=MESH)

    def scoped(f):
        def inner(*a):
            with jax.named_scope(f.__name__):
                return f(*a)

        return inner

    loads = {}

    def load(name, source, target):
        loads[name] = pltpu.make_async_copy(source, target, load_sem.at[len(loads)])
        loads[name].start()

    @scoped
    def arrived(*names):
        for name in names:
            loads[name].wait()

    first = [(320, 448), (192, 320), (64, 192), (0, 64)]
    later = [(384, 448), (256, 384), (128, 256), (0, 128)]

    load("gain", gain_hbm, gain)
    load(("x", 0), x_hbm.at[pl.ds(320, 128)], x.at[pl.ds(320, 128)])
    for k in range(PIECES):
        features = pl.ds(k * (width // PIECES), width // PIECES)
        load(("wv", 0, k), wv_hbm.at[0, features], w.at[0, features, pl.ds(0, half)])
        load(("wg", 0, k), wg_hbm.at[0, features], w.at[0, features, pl.ds(half, half)])
    for i in (1, 2, 3):
        rows = pl.ds(first[i][0], first[i][1] - first[i][0])
        load(("x", i), x_hbm.at[rows], x.at[rows])
    load("fwd", fwd_hbm, fwd)
    load("rev", rev_hbm, rev)
    load("taps", taps_hbm, taps)
    load("inv", inv_hbm, inv)
    load("bias", bias_hbm, bias)
    load("cgain", cgain_hbm, cgain)
    load("cshift", cshift_hbm, cshift)
    load(("wo", 0), wo_hbm.at[0], wo.at[0])
    load(("wv", 1), wv_hbm.at[1], w.at[1, :, pl.ds(0, half)])
    load(("wg", 1), wg_hbm.at[1], w.at[1, :, pl.ds(half, half)])
    load(("wo", 1), wo_hbm.at[1], wo.at[1])

    for layer in range(layers):
        own[layer, pl.ds(tokens, own.shape[1] - tokens), :] = jnp.zeros((own.shape[1] - tokens, half), BF16)

    @pl.when(me == 0)
    def _():
        halo[...] = jnp.zeros_like(halo)

    def chunk(layer, j):
        row = tokens - CHUNK * (j + 1)
        return pltpu.make_async_remote_copy(
            src_ref=own.at[layer, pl.ds(row, CHUNK)],
            dst_ref=halo.at[layer, pl.ds(CHUNK + row, CHUNK)],
            send_sem=send_sem.at[layer, j],
            recv_sem=recv_sem.at[layer, j],
            device_id=(after, core),
            device_id_type=MESH,
        )

    def relay(layer):
        return pltpu.make_async_remote_copy(
            src_ref=halo.at[layer, pl.ds(tokens, CHUNK)],
            dst_ref=halo.at[layer, pl.ds(0, CHUNK)],
            send_sem=relay_send.at[layer],
            recv_sem=relay_recv.at[layer],
            device_id=(after, core),
            device_id_type=MESH,
        )

    def pair(layer, m):
        low, high = later[3 - m]
        rows = pl.ds(low, high - low)
        return pltpu.make_async_remote_copy(
            src_ref=both.at[layer, core, rows],
            dst_ref=both.at[layer, core, rows],
            send_sem=pair_send.at[layer, m],
            recv_sem=pair_recv.at[layer, m],
            device_id=(me, 1 - core),
            device_id_type=MESH,
        )

    def strips(count, step):
        lax.fori_loop(0, count // STRIP, lambda i, c: (step(pl.multiple_of(i * STRIP, STRIP)), c)[1], 0, unroll=True)

    def gate(layer, low, count, scale, mm):
        values, gates = mm[:, :half] * scale, mm[:, half:] * scale
        own[layer, pl.ds(low, count), :] = (values * sigmoid(gates)).astype(BF16)

    def row_scale(squares):
        return lax.rsqrt(jnp.sum(squares, axis=-1, keepdims=True) * (1.0 / width) + 1e-06)

    @scoped
    def prepare(low, high):
        count = high - low

        def step(r):
            values = x[pl.ds(low + r, STRIP), :].astype(F32)
            normed[pl.ds(r, STRIP), :] = (values * gain[pl.ds(0, 1), :]).astype(BF16)
            squares = sum(values[:, at : at + LANES] * values[:, at : at + LANES] for at in range(0, width, LANES))
            scales[pl.ds(r, STRIP), :] = jnp.broadcast_to(row_scale(squares), (STRIP, LANES))

        strips(count, step)

    @scoped
    def project(low, high, pieces=1):
        count = high - low
        mm = 0.0
        for k in range(pieces):
            if pieces > 1:
                arrived(("wv", 0, k), ("wg", 0, k))
            features = pl.ds(k * (width // pieces), width // pieces)
            mm = mm + jnp.dot(normed[pl.ds(0, count), features], w[0, features, :], preferred_element_type=F32)
        scale = scales[pl.ds(0, count), :]
        gate(0, low, count, jnp.concatenate([scale] * (half // LANES), axis=1), mm)

    def send(layer, low, high, who=None):
        @pl.when(has_next if who is None else jnp.logical_and(has_next, core == who))
        def _():
            for j in range((tokens - high) // CHUNK, (tokens - low) // CHUNK):
                chunk(layer, j).start()

    @scoped
    def received(layer, *which):
        @pl.when(has_prev)
        def _():
            for j in which:
                if j < chunks:
                    chunk(layer, j).wait_recv()
                else:
                    relay(layer).wait_recv()

    def send_relay(layer):
        @pl.when(has_next)
        def _():
            relay(layer).start()

    @scoped
    def transform(layer, s):
        if s < 0:
            block = halo[layer, pl.ds(BLOCK * (s + 4), BLOCK), :]
        else:
            block = own[layer, pl.ds(BLOCK * s, BLOCK), :]
        spec[layer, s + 4] = jnp.dot(fwd[...], jnp.concatenate([block, block]), preferred_element_type=F32)

    @scoped
    def tap_spectra(layer):
        for b in range(4):
            block = taps[layer, pl.ds(BLOCK * (3 - b), BLOCK), :]
            lag[b] = jnp.dot(rev[...], jnp.concatenate([block, block]), preferred_element_type=F32)

        def step(i, carry):
            r = pl.multiple_of(i * STRIP, STRIP)
            odd = lax.rem(lax.broadcasted_iota(jnp.int32, (STRIP, half), 0), 2)
            sign = 1.0 - 2.0 * odd.astype(F32)
            re = [lag[b, pl.ds(r, STRIP), :] for b in range(4)]
            im = [lag[b, pl.ds(BLOCK + r, STRIP), :] for b in range(4)]
            for c in range(5):
                new_re, new_im = 0.0, 0.0
                if c < 4:
                    new_re, new_im = sign * im[c], -sign * re[c]
                if c > 0:
                    new_re, new_im = new_re + re[c - 1], new_im + im[c - 1]
                lags[layer, c, pl.ds(r, STRIP), :] = new_re
                lags[layer, c, pl.ds(BLOCK + r, STRIP), :] = new_im
            return carry

        lax.fori_loop(0, BLOCK // STRIP, step, 0, unroll=True)

    def products(layer, m, r, taken):
        y_re, y_im = 0.0, 0.0
        for c in taken:
            h_re, h_im = lags[layer, c, pl.ds(r, STRIP), :], lags[layer, c, pl.ds(BLOCK + r, STRIP), :]
            s = m - c + 4
            a_re, a_im = spec[layer, s, pl.ds(r, STRIP), :], spec[layer, s, pl.ds(BLOCK + r, STRIP), :]
            y_re = y_re + (h_re * a_re - h_im * a_im)
            y_im = y_im + (h_re * a_im + h_im * a_re)
        return y_re, y_im

    @scoped
    def foresee(layer, m):
        def step(r):
            y_re, y_im = products(layer, m, r, range(4))
            part[pl.ds(r, STRIP), :] = y_re
            part[pl.ds(BLOCK + r, STRIP), :] = y_im

        strips(BLOCK, step)

    @scoped
    def convolve(layer, m):
        low, high = later[3 - m]

        def step(r):
            y_re, y_im = products(layer, m, r, (4,))
            y_re, y_im = y_re + part[pl.ds(r, STRIP), :], y_im + part[pl.ds(BLOCK + r, STRIP), :]
            for at, y in ((0, y_re), (BLOCK, y_im)):
                top = y.astype(BF16)
                prod[pl.ds(at + r, STRIP), :] = top
                prod[pl.ds(2 * BLOCK + at + r, STRIP), :] = (y - top.astype(F32)).astype(BF16)

        strips(BLOCK, step)
        rows = pl.ds(0, high - low)
        conv = jnp.dot(inv[rows, pl.ds(0, 4 * BLOCK)], prod[...], preferred_element_type=F32)
        conv += jnp.dot(inv[rows, pl.ds(4 * BLOCK, 2 * BLOCK)], prod[pl.ds(0, 2 * BLOCK), :], preferred_element_type=F32)
        both[layer, core, pl.ds(low, high - low), :] = (conv + bias[pl.ds(layer, 1), :]).astype(BF16)
        pair(layer, m).start()

    @scoped
    def paired(layer, *which):
        for m in which:
            pair(layer, m).wait_recv()

    @scoped
    def mix(layer, m):
        low, high = later[3 - m]

        def step(r):
            rows = pl.ds(low + r, STRIP)
            parts = [both[layer, p, rows, :].astype(F32) for p in range(2)]
            center = jnp.sum(parts[0] + parts[1], axis=-1, keepdims=True) * (0.5 / half)
            parts = [v - center for v in parts]
            spread = jnp.sum(parts[0] * parts[0] + parts[1] * parts[1], axis=-1, keepdims=True) * (0.5 / half)
            scale = lax.rsqrt(spread + 1e-05)
            for p, v in enumerate(parts):
                columns = pl.ds(p * half, half)
                n = v * scale * cgain[pl.ds(layer, 1), columns] + cshift[pl.ds(layer, 1), columns]
                mixed[rows, columns] = (n * sigmoid(n)).astype(BF16)

        strips(high - low, step)

    @scoped
    def finish(layer, *which):
        low, high = min(later[3 - m][0] for m in which), max(later[3 - m][1] for m in which)
        count = high - low
        rows = pl.ds(low, count)
        piece = 512
        squares, mm, ahead = 0.0, 0.0, None

        def widen(at):
            return jnp.dot(mixed[rows, :], wo[layer, :, pl.ds(at, piece)], preferred_element_type=F32)

        update = widen(0)
        for at in range(0, width, piece):
            columns = pl.ds(at, piece)
            if at + piece < width:
                ahead = widen(at + piece)
            state = (x[rows, columns].astype(F32) + update).astype(BF16)
            update = ahead
            if layer == layers - 1:
                out[rows, columns] = state
                continue
            x[rows, columns] = state
            state = state.astype(F32)
            scaled = (state * gain[pl.ds(layer + 1, 1), columns]).astype(BF16)
            mm = mm + jnp.dot(scaled, w[layer + 1, columns, :], preferred_element_type=F32)
            squares = squares + sum(state[:, q : q + LANES] * state[:, q : q + LANES] for q in range(0, piece, LANES))
        if layer < layers - 1:
            gate(layer + 1, low, count, row_scale(squares), mm)
            send(layer + 1, low, high)

    arrived("gain", ("x", 0))
    prepare(*first[0])
    project(*first[0], PIECES)
    with jax.named_scope("barrier"):

        @pl.when(has_next)
        def _():
            pl.semaphore_wait(barrier, 2)

        @pl.when(jnp.logical_not(has_next))
        def _():
            pl.semaphore_wait(barrier, 1)

    send(0, *first[0])
    for i in (1, 2, 3):
        arrived(("x", i))
        prepare(*first[i])
        project(*first[i])
        send(0, *first[i])
    arrived("fwd", "rev", "taps", "inv", "bias", "cgain", "cshift")
    for s in (3, 2, 1, 0):
        transform(0, s)
    tap_spectra(0)
    foresee(0, 3)
    tap_spectra(1)

    for layer in range(layers):
        received(layer, 0, 1)
        send_relay(layer)
        transform(layer, -1)
        convolve(layer, 3)
        foresee(layer, 2)
        received(layer, 2, 3)
        transform(layer, -2)
        convolve(layer, 2)
        if layer == 0:
            arrived(("wo", 0), ("wv", 1), ("wg", 1))
        paired(layer, 3)
        mix(layer, 3)
        foresee(layer, 1)
        finish(layer, 3)
        received(layer, 4, 5)
        transform(layer, -3)
        convolve(layer, 1)
        paired(layer, 2)
        mix(layer, 2)
        foresee(layer, 0)
        finish(layer, 2)
        received(layer, 6, 7)
        transform(layer, -4)
        convolve(layer, 0)
        paired(layer, 1)
        mix(layer, 1)
        if layer == 0:
            transform(1, 3)
            transform(1, 2)
        finish(layer, 1)
        paired(layer, 0)
        mix(layer, 0)
        if layer == 0:
            transform(1, 1)
        finish(layer, 0)
        if layer == 0:
            transform(1, 0)
            foresee(1, 3)
            arrived(("wo", 1))

    for layer in range(layers):
        for m in range(4):
            pair(layer, m).wait_send()

        @pl.when(has_next)
        def _():
            for j in range(chunks):
                chunk(layer, j).wait_send()
            relay(layer).wait_send()


def per_device(
    devices,
    stream,
    norm_gain,
    value_weight,
    gate_weight,
    conv_taps,
    conv_bias,
    channel_gain,
    channel_shift,
    out_weight,
):
    tokens, width = stream.shape
    layers, span, half = conv_taps.shape
    padded = -(-tokens // BLOCK) * BLOCK
    forward, reverse, inverse = (jnp.asarray(m) for m in spectra())
    dma = pltpu.SemaphoreType.DMA
    return pl.pallas_call(
        functools.partial(kernel, devices),
        out_shape=pltpu.VMEM((tokens, width), BF16),
        in_specs=[pl.BlockSpec(memory_space=pltpu.HBM)] * 12,
        out_specs=pl.BlockSpec(memory_space=pltpu.VMEM),
        scratch_shapes=[
            pltpu.VMEM((tokens, width), BF16),
            pltpu.VMEM((layers, width, 2 * half), BF16),
            pltpu.VMEM((layers, 2 * half, width), BF16),
            pltpu.VMEM((layers, span, half), BF16),
            pltpu.VMEM((layers, width), F32),
            pltpu.VMEM((layers, half), F32),
            pltpu.VMEM((layers, 2 * half), F32),
            pltpu.VMEM((layers, 2 * half), F32),
            pltpu.VMEM(forward.shape, BF16),
            pltpu.VMEM(reverse.shape, BF16),
            pltpu.VMEM(inverse.shape, BF16),
            pltpu.VMEM((2 * BLOCK, width), BF16),
            pltpu.VMEM((layers, padded, half), BF16),
            pltpu.VMEM((layers, span, half), BF16),
            pltpu.VMEM((layers, 8, 2 * BLOCK, half), F32),
            pltpu.VMEM((layers, 5, 2 * BLOCK, half), F32),
            pltpu.VMEM((4, 2 * BLOCK, half), F32),
            pltpu.VMEM((4 * BLOCK, half), BF16),
            pltpu.VMEM((2 * BLOCK, half), F32),
            pltpu.VMEM((BLOCK, LANES), F32),
            pltpu.VMEM((layers, 2, tokens, half), BF16),
            pltpu.VMEM((tokens, 2 * half), BF16),
            dma((32,)),
            dma((layers, tokens // CHUNK)),
            dma((layers, tokens // CHUNK)),
            dma((layers,)),
            dma((layers,)),
            dma((layers, 4)),
            dma((layers, 4)),
        ],
        compiler_params=pltpu.CompilerParams(
            collective_id=0, has_side_effects=True, vmem_limit_bytes=60 * 1024 * 1024
        ),
        name="stacked_conv",
    )(
        stream, norm_gain, value_weight, gate_weight, conv_taps, conv_bias, channel_gain, channel_shift, out_weight,
        forward, reverse, inverse,
    )


def solution(mesh):
    return jax.shard_map(
        functools.partial(per_device, mesh.shape["sp"]),
        mesh=mesh,
        in_specs=(
            P("sp", None),
            P(),
            P(None, None, "tp"),
            P(None, None, "tp"),
            P(None, None, "tp"),
            P(None, "tp"),
            P(),
            P(),
            P(),
        ),
        out_specs=P("sp", None),
        check_vma=False,
    )
```

```python
import functools

import jax
import jax.numpy as jnp
import numpy as np
from jax import lax
from jax.experimental import pallas as pl
from jax.experimental.pallas import tpu as pltpu
from jax.sharding import PartitionSpec as P

BLOCK = 128
CHUNK = 64
STRIP = 16
BF16 = jnp.bfloat16
F32 = jnp.float32
LANES = 128
PIECES = 4
MESH = pl.DeviceIdType.MESH


def sigmoid(v):
    return 0.5 * jnp.tanh(0.5 * v) + 0.5


def halves(matrix):
    high = matrix.astype(np.float32).astype(BF16)
    low = (matrix - high.astype(np.float64)).astype(np.float32).astype(BF16)
    return high, low


def spectra():
    odd = 2 * np.arange(BLOCK)[:, None] + 1
    angle = np.pi * odd * np.arange(BLOCK)[None, :] / (2 * BLOCK)
    forward = np.concatenate([np.cos(angle), -np.sin(angle)])
    reverse = forward[:, ::-1]
    angle = angle + np.pi * odd / 2
    inverse = np.concatenate([np.cos(angle), -np.sin(angle)]).T / BLOCK
    high, low = halves(inverse)
    return (
        np.concatenate(halves(forward), axis=1),
        np.concatenate(halves(reverse), axis=1),
        np.concatenate([high, high, low], axis=1),
    )


def kernel(
    devices,
    x_hbm, gain_hbm, wv_hbm, wg_hbm, taps_hbm, bias_hbm, cgain_hbm, cshift_hbm, wo_hbm, fwd_hbm, rev_hbm, inv_hbm,
    out,
    x, w, wo, taps, gain, bias, cgain, cshift, fwd, rev, inv,
    normed, own, halo, spec, lags, lag, prod, part, scales, both, mixed,
    load_sem, send_sem, recv_sem, relay_send, relay_recv, pair_send, pair_recv,
):
    tokens, width = x.shape
    layers = w.shape[0]
    half = w.shape[2] // 2
    chunks = tokens // CHUNK
    me, core = lax.axis_index("sp"), lax.axis_index("tp")
    after, before = lax.rem(me + 1, devices), lax.rem(me + devices - 1, devices)
    has_next, has_prev = me < devices - 1, me > 0

    barrier = pltpu.get_barrier_semaphore()
    pl.semaphore_signal(barrier, inc=1, device_id=(me, 1 - core), device_id_type=MESH)

    @pl.when(has_prev)
    def _():
        pl.semaphore_signal(barrier, inc=1, device_id=(before, core), device_id_type=MESH)

    def scoped(f):
        def inner(*a):
            with jax.named_scope(f.__name__):
                return f(*a)

        return inner

    loads = {}

    def load(name, source, target):
        loads[name] = pltpu.make_async_copy(source, target, load_sem.at[len(loads)])
        loads[name].start()

    @scoped
    def arrived(*names):
        for name in names:
            loads[name].wait()

    first = [(320, 448), (192, 320), (64, 192), (0, 64)]
    later = [(384, 448), (256, 384), (128, 256), (0, 128)]

    load("gain", gain_hbm, gain)
    load(("x", 0), x_hbm.at[pl.ds(320, 128)], x.at[pl.ds(320, 128)])
    for k in range(PIECES):
        features = pl.ds(k * (width // PIECES), width // PIECES)
        load(("wv", 0, k), wv_hbm.at[0, features], w.at[0, features, pl.ds(0, half)])
        load(("wg", 0, k), wg_hbm.at[0, features], w.at[0, features, pl.ds(half, half)])
    for i in (1, 2, 3):
        rows = pl.ds(first[i][0], first[i][1] - first[i][0])
        load(("x", i), x_hbm.at[rows], x.at[rows])
    load("fwd", fwd_hbm, fwd)
    load("rev", rev_hbm, rev)
    load("taps", taps_hbm, taps)
    load("inv", inv_hbm, inv)
    load("bias", bias_hbm, bias)
    load("cgain", cgain_hbm, cgain)
    load("cshift", cshift_hbm, cshift)
    load(("wo", 0), wo_hbm.at[0], wo.at[0])
    load(("wv", 1), wv_hbm.at[1], w.at[1, :, pl.ds(0, half)])
    load(("wg", 1), wg_hbm.at[1], w.at[1, :, pl.ds(half, half)])
    load(("wo", 1), wo_hbm.at[1], wo.at[1])

    for layer in range(layers):
        own[layer, pl.ds(tokens, own.shape[1] - tokens), :] = jnp.zeros((own.shape[1] - tokens, half), BF16)

    @pl.when(me == 0)
    def _():
        halo[...] = jnp.zeros_like(halo)

    def chunk(layer, j):
        row = tokens - CHUNK * (j + 1)
        return pltpu.make_async_remote_copy(
            src_ref=own.at[layer, pl.ds(row, CHUNK)],
            dst_ref=halo.at[layer, pl.ds(CHUNK + row, CHUNK)],
            send_sem=send_sem.at[layer, j],
            recv_sem=recv_sem.at[layer, j],
            device_id=(after, core),
            device_id_type=MESH,
        )

    def relay(layer):
        return pltpu.make_async_remote_copy(
            src_ref=halo.at[layer, pl.ds(tokens, CHUNK)],
            dst_ref=halo.at[layer, pl.ds(0, CHUNK)],
            send_sem=relay_send.at[layer],
            recv_sem=relay_recv.at[layer],
            device_id=(after, core),
            device_id_type=MESH,
        )

    def pair(layer, m):
        low, high = later[3 - m]
        rows = pl.ds(low, high - low)
        return pltpu.make_async_remote_copy(
            src_ref=both.at[layer, core, rows],
            dst_ref=both.at[layer, core, rows],
            send_sem=pair_send.at[layer, m],
            recv_sem=pair_recv.at[layer, m],
            device_id=(me, 1 - core),
            device_id_type=MESH,
        )

    def strips(count, step):
        lax.fori_loop(0, count // STRIP, lambda i, c: (step(pl.multiple_of(i * STRIP, STRIP)), c)[1], 0, unroll=True)

    def gate(layer, low, count, scale, mm):
        values, gates = mm[:, :half] * scale, mm[:, half:] * scale
        own[layer, pl.ds(low, count), :] = (values * sigmoid(gates)).astype(BF16)

    def row_scale(squares):
        return lax.rsqrt(jnp.sum(squares, axis=-1, keepdims=True) * (1.0 / width) + 1e-06)

    @scoped
    def prepare(low, high):
        count = high - low

        def step(r):
            values = x[pl.ds(low + r, STRIP), :].astype(F32)
            normed[pl.ds(r, STRIP), :] = (values * gain[pl.ds(0, 1), :]).astype(BF16)
            squares = sum(values[:, at : at + LANES] * values[:, at : at + LANES] for at in range(0, width, LANES))
            scales[pl.ds(r, STRIP), :] = jnp.broadcast_to(row_scale(squares), (STRIP, LANES))

        strips(count, step)

    @scoped
    def project(low, high, pieces=1):
        count = high - low
        mm = 0.0
        for k in range(pieces):
            if pieces > 1:
                arrived(("wv", 0, k), ("wg", 0, k))
            features = pl.ds(k * (width // pieces), width // pieces)
            mm = mm + jnp.dot(normed[pl.ds(0, count), features], w[0, features, :], preferred_element_type=F32)
        scale = scales[pl.ds(0, count), :]
        gate(0, low, count, jnp.concatenate([scale] * (half // LANES), axis=1), mm)

    def send(layer, low, high, who=None):
        @pl.when(has_next if who is None else jnp.logical_and(has_next, core == who))
        def _():
            for j in range((tokens - high) // CHUNK, (tokens - low) // CHUNK):
                chunk(layer, j).start()

    @scoped
    def received(layer, *which):
        @pl.when(has_prev)
        def _():
            for j in which:
                if j < chunks:
                    chunk(layer, j).wait_recv()
                else:
                    relay(layer).wait_recv()

    def send_relay(layer):
        @pl.when(has_next)
        def _():
            relay(layer).start()

    def transform(layer, s):
        if s < 0:
            block = halo[layer, pl.ds(BLOCK * (s + 4), BLOCK), :]
        else:
            block = own[layer, pl.ds(BLOCK * s, BLOCK), :]
        spec[layer, s + 4] = jnp.dot(fwd[...], jnp.concatenate([block, block]), preferred_element_type=F32)

    @scoped
    def tap_spectra(layer):
        for b in range(4):
            block = taps[layer, pl.ds(BLOCK * (3 - b), BLOCK), :]
            lag[b] = jnp.dot(rev[...], jnp.concatenate([block, block]), preferred_element_type=F32)

        def step(i, carry):
            r = pl.multiple_of(i * STRIP, STRIP)
            odd = lax.rem(lax.broadcasted_iota(jnp.int32, (STRIP, half), 0), 2)
            sign = 1.0 - 2.0 * odd.astype(F32)
            re = [lag[b, pl.ds(r, STRIP), :] for b in range(4)]
            im = [lag[b, pl.ds(BLOCK + r, STRIP), :] for b in range(4)]
            for c in range(5):
                new_re, new_im = 0.0, 0.0
                if c < 4:
                    new_re, new_im = sign * im[c], -sign * re[c]
                if c > 0:
                    new_re, new_im = new_re + re[c - 1], new_im + im[c - 1]
                lags[layer, c, pl.ds(r, STRIP), :] = new_re
                lags[layer, c, pl.ds(BLOCK + r, STRIP), :] = new_im
            return carry

        lax.fori_loop(0, BLOCK // STRIP, step, 0, unroll=True)

    def products(layer, m, r, taken):
        y_re, y_im = 0.0, 0.0
        for c in taken:
            h_re, h_im = lags[layer, c, pl.ds(r, STRIP), :], lags[layer, c, pl.ds(BLOCK + r, STRIP), :]
            s = m - c + 4
            a_re, a_im = spec[layer, s, pl.ds(r, STRIP), :], spec[layer, s, pl.ds(BLOCK + r, STRIP), :]
            y_re = y_re + (h_re * a_re - h_im * a_im)
            y_im = y_im + (h_re * a_im + h_im * a_re)
        return y_re, y_im

    def foresee(layer, m):
        def step(r):
            y_re, y_im = products(layer, m, r, range(4))
            part[m % 2, pl.ds(r, STRIP), :] = y_re
            part[m % 2, pl.ds(BLOCK + r, STRIP), :] = y_im

        strips(BLOCK, step)

    def convolve(layer, m):
        low, high = later[3 - m]

        def step(r):
            y_re, y_im = products(layer, m, r, (4,))
            y_re, y_im = y_re + part[m % 2, pl.ds(r, STRIP), :], y_im + part[m % 2, pl.ds(BLOCK + r, STRIP), :]
            for at, y in ((0, y_re), (BLOCK, y_im)):
                top = y.astype(BF16)
                prod[pl.ds(at + r, STRIP), :] = top
                prod[pl.ds(2 * BLOCK + at + r, STRIP), :] = (y - top.astype(F32)).astype(BF16)

        strips(BLOCK, step)
        rows = pl.ds(0, high - low)
        conv = jnp.dot(inv[rows, pl.ds(0, 4 * BLOCK)], prod[...], preferred_element_type=F32)
        conv += jnp.dot(inv[rows, pl.ds(4 * BLOCK, 2 * BLOCK)], prod[pl.ds(0, 2 * BLOCK), :], preferred_element_type=F32)
        both[layer, core, pl.ds(low, high - low), :] = (conv + bias[pl.ds(layer, 1), :]).astype(BF16)

    @scoped
    def paired(layer, *which):
        for m in which:
            pair(layer, m).wait_recv()

    def mix(layer, m):
        low, high = later[3 - m]

        def step(r):
            rows = pl.ds(low + r, STRIP)
            parts = [both[layer, p, rows, :].astype(F32) for p in range(2)]
            center = jnp.sum(parts[0] + parts[1], axis=-1, keepdims=True) * (0.5 / half)
            parts = [v - center for v in parts]
            spread = jnp.sum(parts[0] * parts[0] + parts[1] * parts[1], axis=-1, keepdims=True) * (0.5 / half)
            scale = lax.rsqrt(spread + 1e-05)
            for p, v in enumerate(parts):
                columns = pl.ds(p * half, half)
                n = v * scale * cgain[pl.ds(layer, 1), columns] + cshift[pl.ds(layer, 1), columns]
                mixed[rows, columns] = (n * sigmoid(n)).astype(BF16)

        strips(high - low, step)

    @scoped
    def finish(layer, *which):
        low, high = min(later[3 - m][0] for m in which), max(later[3 - m][1] for m in which)
        count = high - low
        rows = pl.ds(low, count)
        piece = 512
        squares, mm, ahead = 0.0, 0.0, None

        def widen(at):
            return jnp.dot(mixed[rows, :], wo[layer, :, pl.ds(at, piece)], preferred_element_type=F32)

        update = widen(0)
        for at in range(0, width, piece):
            columns = pl.ds(at, piece)
            if at + piece < width:
                ahead = widen(at + piece)
            state = (x[rows, columns].astype(F32) + update).astype(BF16)
            update = ahead
            if layer == layers - 1:
                out[rows, columns] = state
                continue
            x[rows, columns] = state
            state = state.astype(F32)
            scaled = (state * gain[pl.ds(layer + 1, 1), columns]).astype(BF16)
            mm = mm + jnp.dot(scaled, w[layer + 1, columns, :], preferred_element_type=F32)
            squares = squares + sum(state[:, q : q + LANES] * state[:, q : q + LANES] for q in range(0, piece, LANES))
        if layer < layers - 1:
            gate(layer + 1, low, count, row_scale(squares), mm)
            send(layer + 1, low, high)

    @scoped
    def step(layer, m):
        transform(layer, m - 4)
        convolve(layer, m)
        if m > 0:
            foresee(layer, m - 1)
        pair(layer, m).start()

    @scoped
    def last(layer):
        mix(layer, 0)
        if layer == 0:
            transform(1, 1)
        finish(layer, 0)

    arrived("gain", ("x", 0))
    prepare(*first[0])
    project(*first[0], PIECES)
    with jax.named_scope("barrier"):

        @pl.when(has_next)
        def _():
            pl.semaphore_wait(barrier, 2)

        @pl.when(jnp.logical_not(has_next))
        def _():
            pl.semaphore_wait(barrier, 1)

    send(0, *first[0])
    for i in (1, 2, 3):
        arrived(("x", i))
        prepare(*first[i])
        project(*first[i])
        send(0, *first[i])
    arrived("fwd", "rev", "taps", "inv", "bias", "cgain", "cshift")
    for s in (3, 2, 1, 0):
        transform(0, s)
    tap_spectra(0)
    foresee(0, 3)
    tap_spectra(1)

    for layer in range(layers):
        received(layer, 0, 1)
        send_relay(layer)
        step(layer, 3)
        received(layer, 2, 3)
        step(layer, 2)
        if layer == 0:
            arrived(("wo", 0), ("wv", 1), ("wg", 1))
        paired(layer, 3)
        mix(layer, 3)
        finish(layer, 3)
        received(layer, 4, 5)
        step(layer, 1)
        if layer == layers - 1:
            received(layer, 6, 7)
            step(layer, 0)
        paired(layer, 2)
        mix(layer, 2)
        finish(layer, 2)
        if layer < layers - 1:
            received(layer, 6, 7)
            step(layer, 0)
        paired(layer, 1)
        mix(layer, 1)
        if layer == 0:
            transform(1, 3)
            transform(1, 2)
        finish(layer, 1)
        paired(layer, 0)
        last(layer)
        if layer == 0:
            transform(1, 0)
            foresee(1, 3)
            arrived(("wo", 1))

    for layer in range(layers):
        for m in range(4):
            pair(layer, m).wait_send()

        @pl.when(has_next)
        def _():
            for j in range(chunks):
                chunk(layer, j).wait_send()
            relay(layer).wait_send()


def per_device(
    devices,
    stream,
    norm_gain,
    value_weight,
    gate_weight,
    conv_taps,
    conv_bias,
    channel_gain,
    channel_shift,
    out_weight,
):
    tokens, width = stream.shape
    layers, span, half = conv_taps.shape
    padded = -(-tokens // BLOCK) * BLOCK
    forward, reverse, inverse = (jnp.asarray(m) for m in spectra())
    dma = pltpu.SemaphoreType.DMA
    return pl.pallas_call(
        functools.partial(kernel, devices),
        out_shape=pltpu.VMEM((tokens, width), BF16),
        in_specs=[pl.BlockSpec(memory_space=pltpu.HBM)] * 12,
        out_specs=pl.BlockSpec(memory_space=pltpu.VMEM),
        scratch_shapes=[
            pltpu.VMEM((tokens, width), BF16),
            pltpu.VMEM((layers, width, 2 * half), BF16),
            pltpu.VMEM((layers, 2 * half, width), BF16),
            pltpu.VMEM((layers, span, half), BF16),
            pltpu.VMEM((layers, width), F32),
            pltpu.VMEM((layers, half), F32),
            pltpu.VMEM((layers, 2 * half), F32),
            pltpu.VMEM((layers, 2 * half), F32),
            pltpu.VMEM(forward.shape, BF16),
            pltpu.VMEM(reverse.shape, BF16),
            pltpu.VMEM(inverse.shape, BF16),
            pltpu.VMEM((2 * BLOCK, width), BF16),
            pltpu.VMEM((layers, padded, half), BF16),
            pltpu.VMEM((layers, span, half), BF16),
            pltpu.VMEM((layers, 8, 2 * BLOCK, half), F32),
            pltpu.VMEM((layers, 5, 2 * BLOCK, half), F32),
            pltpu.VMEM((4, 2 * BLOCK, half), F32),
            pltpu.VMEM((4 * BLOCK, half), BF16),
            pltpu.VMEM((2, 2 * BLOCK, half), F32),
            pltpu.VMEM((BLOCK, LANES), F32),
            pltpu.VMEM((layers, 2, tokens, half), BF16),
            pltpu.VMEM((tokens, 2 * half), BF16),
            dma((32,)),
            dma((layers, tokens // CHUNK)),
            dma((layers, tokens // CHUNK)),
            dma((layers,)),
            dma((layers,)),
            dma((layers, 4)),
            dma((layers, 4)),
        ],
        compiler_params=pltpu.CompilerParams(
            collective_id=0, has_side_effects=True, vmem_limit_bytes=60 * 1024 * 1024
        ),
        name="stacked_conv",
    )(
        stream, norm_gain, value_weight, gate_weight, conv_taps, conv_bias, channel_gain, channel_shift, out_weight,
        forward, reverse, inverse,
    )


def solution(mesh):
    return jax.shard_map(
        functools.partial(per_device, mesh.shape["sp"]),
        mesh=mesh,
        in_specs=(
            P("sp", None),
            P(),
            P(None, None, "tp"),
            P(None, None, "tp"),
            P(None, None, "tp"),
            P(None, "tp"),
            P(),
            P(),
            P(),
        ),
        out_specs=P("sp", None),
        check_vma=False,
    )
```

```python
import functools

import jax
import jax.numpy as jnp
import numpy as np
from jax import lax
from jax.experimental import pallas as pl
from jax.experimental.pallas import tpu as pltpu
from jax.sharding import PartitionSpec as P

BLOCK = 128
CHUNK = 64
STRIP = 16
BF16 = jnp.bfloat16
F32 = jnp.float32
LANES = 128
PIECES = 4
MESH = pl.DeviceIdType.MESH


def sigmoid(v):
    return 0.5 * jnp.tanh(0.5 * v) + 0.5


def halves(matrix):
    high = matrix.astype(np.float32).astype(BF16)
    low = (matrix - high.astype(np.float64)).astype(np.float32).astype(BF16)
    return high, low


def spectra():
    odd = 2 * np.arange(BLOCK)[:, None] + 1
    angle = np.pi * odd * np.arange(BLOCK)[None, :] / (2 * BLOCK)
    forward = np.concatenate([np.cos(angle), -np.sin(angle)])
    reverse = forward[:, ::-1]
    angle = angle + np.pi * odd / 2
    inverse = np.concatenate([np.cos(angle), -np.sin(angle)]).T / BLOCK
    high, low = halves(inverse)
    return (
        np.concatenate(halves(forward), axis=1),
        np.concatenate(halves(reverse), axis=1),
        np.concatenate([high, high, low], axis=1),
    )


def kernel(
    devices,
    x_hbm, gain_hbm, wv_hbm, wg_hbm, taps_hbm, bias_hbm, cgain_hbm, cshift_hbm, wo_hbm, fwd_hbm, rev_hbm, inv_hbm,
    out, mixed_out, wo_out,
    x, w, wo, taps, gain, bias, cgain, cshift, fwd, rev, inv,
    normed, own, halo, spec, lags, lag, prod, part, scales, both, mixed,
    load_sem, send_sem, recv_sem, relay_send, relay_recv, pair_send, pair_recv,
):
    tokens, width = x.shape
    layers = w.shape[0]
    half = w.shape[2] // 2
    chunks = tokens // CHUNK
    me, core = lax.axis_index("sp"), lax.axis_index("tp")
    after, before = lax.rem(me + 1, devices), lax.rem(me + devices - 1, devices)
    has_next, has_prev = me < devices - 1, me > 0

    barrier = pltpu.get_barrier_semaphore()
    pl.semaphore_signal(barrier, inc=1, device_id=(me, 1 - core), device_id_type=MESH)

    @pl.when(has_prev)
    def _():
        pl.semaphore_signal(barrier, inc=1, device_id=(before, core), device_id_type=MESH)

    def scoped(f):
        def inner(*a):
            with jax.named_scope(f.__name__):
                return f(*a)

        return inner

    loads = {}

    def load(name, source, target):
        loads[name] = pltpu.make_async_copy(source, target, load_sem.at[len(loads)])
        loads[name].start()

    @scoped
    def arrived(*names):
        for name in names:
            loads[name].wait()

    first = [(320, 448), (192, 320), (64, 192), (0, 64)]
    later = [(384, 448), (256, 384), (128, 256), (0, 128)]

    load("gain", gain_hbm, gain)
    load(("x", 0), x_hbm.at[pl.ds(320, 128)], x.at[pl.ds(320, 128)])
    for k in range(PIECES):
        features = pl.ds(k * (width // PIECES), width // PIECES)
        load(("wv", 0, k), wv_hbm.at[0, features], w.at[0, features, pl.ds(0, half)])
        load(("wg", 0, k), wg_hbm.at[0, features], w.at[0, features, pl.ds(half, half)])
    for i in (1, 2, 3):
        rows = pl.ds(first[i][0], first[i][1] - first[i][0])
        load(("x", i), x_hbm.at[rows], x.at[rows])
    load("fwd", fwd_hbm, fwd)
    load("rev", rev_hbm, rev)
    load("taps", taps_hbm, taps)
    load("inv", inv_hbm, inv)
    load("bias", bias_hbm, bias)
    load("cgain", cgain_hbm, cgain)
    load("cshift", cshift_hbm, cshift)
    load(("wo", 0), wo_hbm.at[0], wo)
    load(("wv", 1), wv_hbm.at[1], w.at[1, :, pl.ds(0, half)])
    load(("wg", 1), wg_hbm.at[1], w.at[1, :, pl.ds(half, half)])
    load(("wo", 1), wo_hbm.at[1], wo_out)

    for layer in range(layers):
        own[layer, pl.ds(tokens, own.shape[1] - tokens), :] = jnp.zeros((own.shape[1] - tokens, half), BF16)

    @pl.when(me == 0)
    def _():
        halo[...] = jnp.zeros_like(halo)

    def chunk(layer, j):
        row = tokens - CHUNK * (j + 1)
        return pltpu.make_async_remote_copy(
            src_ref=own.at[layer, pl.ds(row, CHUNK)],
            dst_ref=halo.at[layer, pl.ds(CHUNK + row, CHUNK)],
            send_sem=send_sem.at[layer, j],
            recv_sem=recv_sem.at[layer, j],
            device_id=(after, core),
            device_id_type=MESH,
        )

    def relay(layer):
        return pltpu.make_async_remote_copy(
            src_ref=halo.at[layer, pl.ds(tokens, CHUNK)],
            dst_ref=halo.at[layer, pl.ds(0, CHUNK)],
            send_sem=relay_send.at[layer],
            recv_sem=relay_recv.at[layer],
            device_id=(after, core),
            device_id_type=MESH,
        )

    def pair(layer, m):
        low, high = later[3 - m]
        rows = pl.ds(low, high - low)
        return pltpu.make_async_remote_copy(
            src_ref=both.at[layer, core, rows],
            dst_ref=both.at[layer, core, rows],
            send_sem=pair_send.at[layer, m],
            recv_sem=pair_recv.at[layer, m],
            device_id=(me, 1 - core),
            device_id_type=MESH,
        )

    def strips(count, step):
        lax.fori_loop(0, count // STRIP, lambda i, c: (step(pl.multiple_of(i * STRIP, STRIP)), c)[1], 0, unroll=True)

    def gate(layer, low, count, scale, mm):
        values, gates = mm[:, :half] * scale, mm[:, half:] * scale
        own[layer, pl.ds(low, count), :] = (values * sigmoid(gates)).astype(BF16)

    def row_scale(squares):
        return lax.rsqrt(jnp.sum(squares, axis=-1, keepdims=True) * (1.0 / width) + 1e-06)

    @scoped
    def prepare(low, high):
        count = high - low

        def step(r):
            values = x[pl.ds(low + r, STRIP), :].astype(F32)
            normed[pl.ds(r, STRIP), :] = (values * gain[pl.ds(0, 1), :]).astype(BF16)
            squares = sum(values[:, at : at + LANES] * values[:, at : at + LANES] for at in range(0, width, LANES))
            scales[pl.ds(r, STRIP), :] = jnp.broadcast_to(row_scale(squares), (STRIP, LANES))

        strips(count, step)

    @scoped
    def project(low, high, pieces=1):
        count = high - low
        mm = 0.0
        for k in range(pieces):
            if pieces > 1:
                arrived(("wv", 0, k), ("wg", 0, k))
            features = pl.ds(k * (width // pieces), width // pieces)
            mm = mm + jnp.dot(normed[pl.ds(0, count), features], w[0, features, :], preferred_element_type=F32)
        scale = scales[pl.ds(0, count), :]
        gate(0, low, count, jnp.concatenate([scale] * (half // LANES), axis=1), mm)

    def send(layer, low, high, who=None):
        @pl.when(has_next if who is None else jnp.logical_and(has_next, core == who))
        def _():
            for j in range((tokens - high) // CHUNK, (tokens - low) // CHUNK):
                chunk(layer, j).start()

    @scoped
    def received(layer, *which):
        @pl.when(has_prev)
        def _():
            for j in which:
                if j < chunks:
                    chunk(layer, j).wait_recv()
                else:
                    relay(layer).wait_recv()

    def send_relay(layer):
        @pl.when(has_next)
        def _():
            relay(layer).start()

    def transform(layer, s):
        if s < 0:
            block = halo[layer, pl.ds(BLOCK * (s + 4), BLOCK), :]
        else:
            block = own[layer, pl.ds(BLOCK * s, BLOCK), :]
        spec[layer, s + 4] = jnp.dot(fwd[...], jnp.concatenate([block, block]), preferred_element_type=F32)

    @scoped
    def tap_spectra(layer):
        for b in range(4):
            block = taps[layer, pl.ds(BLOCK * (3 - b), BLOCK), :]
            lag[b] = jnp.dot(rev[...], jnp.concatenate([block, block]), preferred_element_type=F32)

        def step(i, carry):
            r = pl.multiple_of(i * STRIP, STRIP)
            odd = lax.rem(lax.broadcasted_iota(jnp.int32, (STRIP, half), 0), 2)
            sign = 1.0 - 2.0 * odd.astype(F32)
            re = [lag[b, pl.ds(r, STRIP), :] for b in range(4)]
            im = [lag[b, pl.ds(BLOCK + r, STRIP), :] for b in range(4)]
            for c in range(5):
                new_re, new_im = 0.0, 0.0
                if c < 4:
                    new_re, new_im = sign * im[c], -sign * re[c]
                if c > 0:
                    new_re, new_im = new_re + re[c - 1], new_im + im[c - 1]
                lags[layer, c, pl.ds(r, STRIP), :] = new_re
                lags[layer, c, pl.ds(BLOCK + r, STRIP), :] = new_im
            return carry

        lax.fori_loop(0, BLOCK // STRIP, step, 0, unroll=True)

    def products(layer, m, r, taken):
        y_re, y_im = 0.0, 0.0
        for c in taken:
            h_re, h_im = lags[layer, c, pl.ds(r, STRIP), :], lags[layer, c, pl.ds(BLOCK + r, STRIP), :]
            s = m - c + 4
            a_re, a_im = spec[layer, s, pl.ds(r, STRIP), :], spec[layer, s, pl.ds(BLOCK + r, STRIP), :]
            y_re = y_re + (h_re * a_re - h_im * a_im)
            y_im = y_im + (h_re * a_im + h_im * a_re)
        return y_re, y_im

    def foresee(layer, m):
        def step(r):
            y_re, y_im = products(layer, m, r, range(4))
            part[m % 2, pl.ds(r, STRIP), :] = y_re
            part[m % 2, pl.ds(BLOCK + r, STRIP), :] = y_im

        strips(BLOCK, step)

    def convolve(layer, m):
        low, high = later[3 - m]

        def step(r):
            y_re, y_im = products(layer, m, r, (4,))
            y_re, y_im = y_re + part[m % 2, pl.ds(r, STRIP), :], y_im + part[m % 2, pl.ds(BLOCK + r, STRIP), :]
            for at, y in ((0, y_re), (BLOCK, y_im)):
                top = y.astype(BF16)
                prod[pl.ds(at + r, STRIP), :] = top
                prod[pl.ds(2 * BLOCK + at + r, STRIP), :] = (y - top.astype(F32)).astype(BF16)

        strips(BLOCK, step)
        rows = pl.ds(0, high - low)
        conv = jnp.dot(inv[rows, pl.ds(0, 4 * BLOCK)], prod[...], preferred_element_type=F32)
        conv += jnp.dot(inv[rows, pl.ds(4 * BLOCK, 2 * BLOCK)], prod[pl.ds(0, 2 * BLOCK), :], preferred_element_type=F32)
        both[layer, core, pl.ds(low, high - low), :] = (conv + bias[pl.ds(layer, 1), :]).astype(BF16)

    @scoped
    def paired(layer, *which):
        for m in which:
            pair(layer, m).wait_recv()

    def mix(layer, m):
        low, high = later[3 - m]
        target = mixed_out if layer == layers - 1 and m == 0 else mixed

        def step(r):
            rows = pl.ds(low + r, STRIP)
            parts = [both[layer, p, rows, :].astype(F32) for p in range(2)]
            center = jnp.sum(parts[0] + parts[1], axis=-1, keepdims=True) * (0.5 / half)
            parts = [v - center for v in parts]
            spread = jnp.sum(parts[0] * parts[0] + parts[1] * parts[1], axis=-1, keepdims=True) * (0.5 / half)
            scale = lax.rsqrt(spread + 1e-05)
            for p, v in enumerate(parts):
                columns = pl.ds(p * half, half)
                n = v * scale * cgain[pl.ds(layer, 1), columns] + cshift[pl.ds(layer, 1), columns]
                target[rows, columns] = (n * sigmoid(n)).astype(BF16)

        strips(high - low, step)

    @scoped
    def finish(layer, *which):
        low, high = min(later[3 - m][0] for m in which), max(later[3 - m][1] for m in which)
        count = high - low
        rows = pl.ds(low, count)
        piece = 512
        squares, mm, ahead = 0.0, 0.0, None

        def widen(at):
            return jnp.dot(mixed[rows, :], (wo, wo_out)[layer][:, pl.ds(at, piece)], preferred_element_type=F32)

        update = widen(0)
        for at in range(0, width, piece):
            columns = pl.ds(at, piece)
            if at + piece < width:
                ahead = widen(at + piece)
            state = (x[rows, columns].astype(F32) + update).astype(BF16)
            update = ahead
            if layer == layers - 1:
                out[rows, columns] = state
                continue
            x[rows, columns] = state
            if low == 0:
                out[rows, columns] = state
            state = state.astype(F32)
            scaled = (state * gain[pl.ds(layer + 1, 1), columns]).astype(BF16)
            mm = mm + jnp.dot(scaled, w[layer + 1, columns, :], preferred_element_type=F32)
            squares = squares + sum(state[:, q : q + LANES] * state[:, q : q + LANES] for q in range(0, piece, LANES))
        if layer < layers - 1:
            gate(layer + 1, low, count, row_scale(squares), mm)
            send(layer + 1, low, high)

    @scoped
    def step(layer, m):
        transform(layer, m - 4)
        convolve(layer, m)
        if m > 0:
            foresee(layer, m - 1)
        pair(layer, m).start()

    @scoped
    def last(layer):
        mix(layer, 0)
        if layer == 0:
            transform(1, 1)
        if layer < layers - 1:
            finish(layer, 0)

    arrived("gain", ("x", 0))
    prepare(*first[0])
    project(*first[0], PIECES)
    with jax.named_scope("barrier"):

        @pl.when(has_next)
        def _():
            pl.semaphore_wait(barrier, 2)

        @pl.when(jnp.logical_not(has_next))
        def _():
            pl.semaphore_wait(barrier, 1)

    send(0, *first[0])
    for i in (1, 2, 3):
        arrived(("x", i))
        prepare(*first[i])
        project(*first[i])
        send(0, *first[i])
    arrived("fwd", "rev", "taps", "inv", "bias", "cgain", "cshift")
    for s in (3, 2, 1, 0):
        transform(0, s)
    tap_spectra(0)
    foresee(0, 3)
    tap_spectra(1)

    for layer in range(layers):
        received(layer, 0, 1)
        send_relay(layer)
        step(layer, 3)
        received(layer, 2, 3)
        step(layer, 2)
        if layer == 0:
            arrived(("wo", 0), ("wv", 1), ("wg", 1))
        paired(layer, 3)
        mix(layer, 3)
        finish(layer, 3)
        received(layer, 4, 5)
        step(layer, 1)
        if layer == layers - 1:
            received(layer, 6, 7)
            step(layer, 0)
        paired(layer, 2)
        mix(layer, 2)
        finish(layer, 2)
        if layer < layers - 1:
            received(layer, 6, 7)
            step(layer, 0)
        paired(layer, 1)
        mix(layer, 1)
        if layer == 0:
            transform(1, 3)
            transform(1, 2)
        finish(layer, 1)
        paired(layer, 0)
        last(layer)
        if layer == 0:
            transform(1, 0)
            foresee(1, 3)
            arrived(("wo", 1))

    for layer in range(layers):
        for m in range(4):
            pair(layer, m).wait_send()

        @pl.when(has_next)
        def _():
            for j in range(chunks):
                chunk(layer, j).wait_send()
            relay(layer).wait_send()


def close(result, mixed, wo, out_hbm, block, sem):
    tokens, width = result.shape
    count = mixed.shape[0]
    rest = pl.ds(count, tokens - count)
    copies = [pltpu.make_async_copy(result.at[rest], out_hbm.at[rest], sem.at[0])]
    copies[0].start()
    piece = 512
    for i, at in enumerate(range(0, width, piece)):
        columns = pl.ds(at, piece)
        update = jnp.dot(mixed[...], wo[:, columns], preferred_element_type=F32)
        block[:, columns] = (result[pl.ds(0, count), columns].astype(F32) + update).astype(BF16)
        copies.append(
            pltpu.make_async_copy(block.at[:, columns], out_hbm.at[pl.ds(0, count), columns], sem.at[1 + i])
        )
        copies[-1].start()
    for copy in copies:
        copy.wait()


def per_device(
    devices,
    stream,
    norm_gain,
    value_weight,
    gate_weight,
    conv_taps,
    conv_bias,
    channel_gain,
    channel_shift,
    out_weight,
):
    tokens, width = stream.shape
    layers, span, half = conv_taps.shape
    padded = -(-tokens // BLOCK) * BLOCK
    forward, reverse, inverse = (jnp.asarray(m) for m in spectra())
    dma = pltpu.SemaphoreType.DMA
    result, mixed, wo = pl.pallas_call(
        functools.partial(kernel, devices),
        out_shape=(
            pltpu.VMEM((tokens, width), BF16),
            pltpu.VMEM((BLOCK, 2 * half), BF16),
            pltpu.VMEM((2 * half, width), BF16),
        ),
        in_specs=[pl.BlockSpec(memory_space=pltpu.HBM)] * 12,
        out_specs=[pl.BlockSpec(memory_space=pltpu.VMEM)] * 3,
        scratch_shapes=[
            pltpu.VMEM((tokens, width), BF16),
            pltpu.VMEM((layers, width, 2 * half), BF16),
            pltpu.VMEM((2 * half, width), BF16),
            pltpu.VMEM((layers, span, half), BF16),
            pltpu.VMEM((layers, width), F32),
            pltpu.VMEM((layers, half), F32),
            pltpu.VMEM((layers, 2 * half), F32),
            pltpu.VMEM((layers, 2 * half), F32),
            pltpu.VMEM(forward.shape, BF16),
            pltpu.VMEM(reverse.shape, BF16),
            pltpu.VMEM(inverse.shape, BF16),
            pltpu.VMEM((2 * BLOCK, width), BF16),
            pltpu.VMEM((layers, padded, half), BF16),
            pltpu.VMEM((layers, span, half), BF16),
            pltpu.VMEM((layers, 8, 2 * BLOCK, half), F32),
            pltpu.VMEM((layers, 5, 2 * BLOCK, half), F32),
            pltpu.VMEM((4, 2 * BLOCK, half), F32),
            pltpu.VMEM((4 * BLOCK, half), BF16),
            pltpu.VMEM((2, 2 * BLOCK, half), F32),
            pltpu.VMEM((BLOCK, LANES), F32),
            pltpu.VMEM((layers, 2, tokens, half), BF16),
            pltpu.VMEM((tokens, 2 * half), BF16),
            dma((32,)),
            dma((layers, tokens // CHUNK)),
            dma((layers, tokens // CHUNK)),
            dma((layers,)),
            dma((layers,)),
            dma((layers, 4)),
            dma((layers, 4)),
        ],
        compiler_params=pltpu.CompilerParams(
            collective_id=0, has_side_effects=True, vmem_limit_bytes=59 * 1024 * 1024
        ),
        name="stacked_conv",
    )(
        stream, norm_gain, value_weight, gate_weight, conv_taps, conv_bias, channel_gain, channel_shift, out_weight,
        forward, reverse, inverse,
    )
    return pl.pallas_call(
        close,
        out_shape=jax.ShapeDtypeStruct((tokens, width), BF16),
        in_specs=[pl.BlockSpec(memory_space=pltpu.VMEM)] * 3,
        out_specs=pl.BlockSpec(memory_space=pl.ANY),
        scratch_shapes=[pltpu.VMEM((BLOCK, width), BF16), dma((5,))],
        compiler_params=pltpu.CompilerParams(vmem_limit_bytes=16 * 1024 * 1024),
        name="close",
    )(result, mixed, wo)


def solution(mesh):
    return jax.shard_map(
        functools.partial(per_device, mesh.shape["sp"]),
        mesh=mesh,
        in_specs=(
            P("sp", None),
            P(),
            P(None, None, "tp"),
            P(None, None, "tp"),
            P(None, None, "tp"),
            P(None, "tp"),
            P(),
            P(),
            P(),
        ),
        out_specs=P("sp", None),
        check_vma=False,
    )
```

```python
import functools

import jax
import jax.numpy as jnp
import numpy as np
from jax import lax
from jax.experimental import pallas as pl
from jax.experimental.pallas import tpu as pltpu
from jax.sharding import PartitionSpec as P

BLOCK = 128
CHUNK = 64
STRIP = 16
BF16 = jnp.bfloat16
F32 = jnp.float32
LANES = 128
PIECES = 8
MESH = pl.DeviceIdType.MESH


def sigmoid(v):
    return 0.5 * jnp.tanh(0.5 * v) + 0.5


def halves(matrix):
    high = matrix.astype(np.float32).astype(BF16)
    low = (matrix - high.astype(np.float64)).astype(np.float32).astype(BF16)
    return high, low


def spectra():
    odd = 2 * np.arange(BLOCK)[:, None] + 1
    angle = np.pi * odd * np.arange(BLOCK)[None, :] / (2 * BLOCK)
    forward = np.concatenate([np.cos(angle), -np.sin(angle)])
    reverse = forward[:, ::-1]
    angle = angle + np.pi * odd / 2
    inverse = np.concatenate([np.cos(angle), -np.sin(angle)]).T / BLOCK
    high, low = halves(inverse)
    return (
        np.concatenate(halves(forward), axis=1),
        np.concatenate(halves(reverse), axis=1),
        np.concatenate([high, high, low], axis=1),
    )


def kernel(
    devices,
    x_hbm, gain_hbm, wv_hbm, wg_hbm, taps_hbm, bias_hbm, cgain_hbm, cshift_hbm, wo_hbm, fwd_hbm, rev_hbm, inv_hbm,
    out, mixed_out, wo_out,
    x, w, wo, taps, gain, bias, cgain, cshift, fwd, rev, inv,
    normed, own, halo, spec, lags, lag, prod, part, scales, both, mixed,
    load_sem, send_sem, recv_sem, relay_send, relay_recv, pair_send, pair_recv,
):
    tokens, width = x.shape
    layers = w.shape[0]
    half = w.shape[2] // 2
    chunks = tokens // CHUNK
    me, core = lax.axis_index("sp"), lax.axis_index("tp")
    after, before = lax.rem(me + 1, devices), lax.rem(me + devices - 1, devices)
    has_next, has_prev = me < devices - 1, me > 0

    barrier = pltpu.get_barrier_semaphore()
    pl.semaphore_signal(barrier, inc=1, device_id=(me, 1 - core), device_id_type=MESH)

    @pl.when(has_prev)
    def _():
        pl.semaphore_signal(barrier, inc=1, device_id=(before, core), device_id_type=MESH)

    def scoped(f):
        def inner(*a):
            with jax.named_scope(f.__name__):
                return f(*a)

        return inner

    loads = {}

    def load(name, source, target):
        loads[name] = pltpu.make_async_copy(source, target, load_sem.at[len(loads)])
        loads[name].start()

    @scoped
    def arrived(*names):
        for name in names:
            loads[name].wait()

    first = [(320, 448), (192, 320), (64, 192), (0, 64)]
    later = [(384, 448), (256, 384), (128, 256), (0, 128)]

    load("gain", gain_hbm, gain)
    load(("x", 0), x_hbm.at[pl.ds(320, 128)], x.at[pl.ds(320, 128)])
    for k in range(PIECES):
        features = pl.ds(k * (width // PIECES), width // PIECES)
        load(("wv", 0, k), wv_hbm.at[0, features], w.at[0, features, pl.ds(0, half)])
        load(("wg", 0, k), wg_hbm.at[0, features], w.at[0, features, pl.ds(half, half)])
    for i in (1, 2, 3):
        rows = pl.ds(first[i][0], first[i][1] - first[i][0])
        load(("x", i), x_hbm.at[rows], x.at[rows])
    load("fwd", fwd_hbm, fwd)
    load("rev", rev_hbm, rev)
    load("taps", taps_hbm, taps)
    load("inv", inv_hbm, inv)
    load("bias", bias_hbm, bias)
    load("cgain", cgain_hbm, cgain)
    load("cshift", cshift_hbm, cshift)
    load(("wo", 0), wo_hbm.at[0], wo)
    load(("wv", 1), wv_hbm.at[1], w.at[1, :, pl.ds(0, half)])
    load(("wg", 1), wg_hbm.at[1], w.at[1, :, pl.ds(half, half)])
    load(("wo", 1), wo_hbm.at[1], wo_out)

    for layer in range(layers):
        own[layer, pl.ds(tokens, own.shape[1] - tokens), :] = jnp.zeros((own.shape[1] - tokens, half), BF16)

    @pl.when(me == 0)
    def _():
        halo[...] = jnp.zeros_like(halo)

    def chunk(layer, j):
        row = tokens - CHUNK * (j + 1)
        return pltpu.make_async_remote_copy(
            src_ref=own.at[layer, pl.ds(row, CHUNK)],
            dst_ref=halo.at[layer, pl.ds(CHUNK + row, CHUNK)],
            send_sem=send_sem.at[layer, j],
            recv_sem=recv_sem.at[layer, j],
            device_id=(after, core),
            device_id_type=MESH,
        )

    def relay(layer):
        return pltpu.make_async_remote_copy(
            src_ref=halo.at[layer, pl.ds(tokens, CHUNK)],
            dst_ref=halo.at[layer, pl.ds(0, CHUNK)],
            send_sem=relay_send.at[layer],
            recv_sem=relay_recv.at[layer],
            device_id=(after, core),
            device_id_type=MESH,
        )

    def pair(layer, m):
        low, high = later[3 - m]
        rows = pl.ds(low, high - low)
        return pltpu.make_async_remote_copy(
            src_ref=both.at[layer, core, rows],
            dst_ref=both.at[layer, core, rows],
            send_sem=pair_send.at[layer, m],
            recv_sem=pair_recv.at[layer, m],
            device_id=(me, 1 - core),
            device_id_type=MESH,
        )

    def strips(count, step):
        lax.fori_loop(0, count // STRIP, lambda i, c: (step(pl.multiple_of(i * STRIP, STRIP)), c)[1], 0, unroll=True)

    def gate(layer, low, count, scale, mm):
        values, gates = mm[:, :half] * scale, mm[:, half:] * scale
        own[layer, pl.ds(low, count), :] = (values * sigmoid(gates)).astype(BF16)

    def row_scale(squares):
        return lax.rsqrt(jnp.sum(squares, axis=-1, keepdims=True) * (1.0 / width) + 1e-06)

    @scoped
    def prepare(low, high):
        count = high - low

        def step(r):
            values = x[pl.ds(low + r, STRIP), :].astype(F32)
            normed[pl.ds(r, STRIP), :] = (values * gain[pl.ds(0, 1), :]).astype(BF16)
            squares = sum(values[:, at : at + LANES] * values[:, at : at + LANES] for at in range(0, width, LANES))
            scales[pl.ds(r, STRIP), :] = jnp.broadcast_to(row_scale(squares), (STRIP, LANES))

        strips(count, step)

    @scoped
    def project(low, high, pieces=1):
        count = high - low
        mm = 0.0
        for k in range(pieces):
            if pieces > 1:
                arrived(("wv", 0, k), ("wg", 0, k))
            features = pl.ds(k * (width // pieces), width // pieces)
            mm = mm + jnp.dot(normed[pl.ds(0, count), features], w[0, features, :], preferred_element_type=F32)
        scale = scales[pl.ds(0, count), :]
        gate(0, low, count, jnp.concatenate([scale] * (half // LANES), axis=1), mm)

    def send(layer, low, high, who=None):
        @pl.when(has_next if who is None else jnp.logical_and(has_next, core == who))
        def _():
            for j in range((tokens - high) // CHUNK, (tokens - low) // CHUNK):
                chunk(layer, j).start()

    @scoped
    def received(layer, *which):
        @pl.when(has_prev)
        def _():
            for j in which:
                if j < chunks:
                    chunk(layer, j).wait_recv()
                else:
                    relay(layer).wait_recv()

    def send_relay(layer):
        @pl.when(has_next)
        def _():
            relay(layer).start()

    def transform(layer, s):
        if s < 0:
            block = halo[layer, pl.ds(BLOCK * (s + 4), BLOCK), :]
        else:
            block = own[layer, pl.ds(BLOCK * s, BLOCK), :]
        twice = jnp.concatenate([block, block])
        for at in (0, BLOCK):
            rows = pl.ds(at, BLOCK)
            spec[layer, s + 4, rows, :] = jnp.dot(fwd[rows, :], twice, preferred_element_type=F32)

    @scoped
    def tap_spectra(layer):
        for b in range(4):
            block = taps[layer, pl.ds(BLOCK * (3 - b), BLOCK), :]
            lag[b] = jnp.dot(rev[...], jnp.concatenate([block, block]), preferred_element_type=F32)

        def step(i, carry):
            r = pl.multiple_of(i * STRIP, STRIP)
            odd = lax.rem(lax.broadcasted_iota(jnp.int32, (STRIP, half), 0), 2)
            sign = 1.0 - 2.0 * odd.astype(F32)
            re = [lag[b, pl.ds(r, STRIP), :] for b in range(4)]
            im = [lag[b, pl.ds(BLOCK + r, STRIP), :] for b in range(4)]
            for c in range(5):
                new_re, new_im = 0.0, 0.0
                if c < 4:
                    new_re, new_im = sign * im[c], -sign * re[c]
                if c > 0:
                    new_re, new_im = new_re + re[c - 1], new_im + im[c - 1]
                lags[layer, c, pl.ds(r, STRIP), :] = new_re
                lags[layer, c, pl.ds(BLOCK + r, STRIP), :] = new_im
            return carry

        lax.fori_loop(0, BLOCK // STRIP, step, 0, unroll=True)

    def products(layer, m, r, taken):
        y_re, y_im = 0.0, 0.0
        for c in taken:
            h_re, h_im = lags[layer, c, pl.ds(r, STRIP), :], lags[layer, c, pl.ds(BLOCK + r, STRIP), :]
            s = m - c + 4
            a_re, a_im = spec[layer, s, pl.ds(r, STRIP), :], spec[layer, s, pl.ds(BLOCK + r, STRIP), :]
            y_re = y_re + (h_re * a_re - h_im * a_im)
            y_im = y_im + (h_re * a_im + h_im * a_re)
        return y_re, y_im

    def foresee(layer, m):
        def step(r):
            y_re, y_im = products(layer, m, r, range(4))
            part[m % 2, pl.ds(r, STRIP), :] = y_re
            part[m % 2, pl.ds(BLOCK + r, STRIP), :] = y_im

        strips(BLOCK, step)

    def convolve(layer, m):
        low, high = later[3 - m]

        def step(r):
            y_re, y_im = products(layer, m, r, (4,))
            y_re, y_im = y_re + part[m % 2, pl.ds(r, STRIP), :], y_im + part[m % 2, pl.ds(BLOCK + r, STRIP), :]
            for at, y in ((0, y_re), (BLOCK, y_im)):
                top = y.astype(BF16)
                prod[pl.ds(at + r, STRIP), :] = top
                prod[pl.ds(2 * BLOCK + at + r, STRIP), :] = (y - top.astype(F32)).astype(BF16)

        strips(BLOCK, step)
        rows = pl.ds(0, high - low)
        conv = jnp.dot(inv[rows, pl.ds(0, 4 * BLOCK)], prod[...], preferred_element_type=F32)
        conv += jnp.dot(inv[rows, pl.ds(4 * BLOCK, 2 * BLOCK)], prod[pl.ds(0, 2 * BLOCK), :], preferred_element_type=F32)
        both[layer, core, pl.ds(low, high - low), :] = (conv + bias[pl.ds(layer, 1), :]).astype(BF16)

    @scoped
    def paired(layer, *which):
        for m in which:
            pair(layer, m).wait_recv()

    def mix(layer, m):
        low, high = later[3 - m]
        target = mixed_out if layer == layers - 1 and m == 0 else mixed

        def step(r):
            rows = pl.ds(low + r, STRIP)
            parts = [both[layer, p, rows, :].astype(F32) for p in range(2)]
            center = jnp.sum(parts[0] + parts[1], axis=-1, keepdims=True) * (0.5 / half)
            parts = [v - center for v in parts]
            spread = jnp.sum(parts[0] * parts[0] + parts[1] * parts[1], axis=-1, keepdims=True) * (0.5 / half)
            scale = lax.rsqrt(spread + 1e-05)
            for p, v in enumerate(parts):
                columns = pl.ds(p * half, half)
                n = v * scale * cgain[pl.ds(layer, 1), columns] + cshift[pl.ds(layer, 1), columns]
                target[rows, columns] = (n * sigmoid(n)).astype(BF16)

        strips(high - low, step)

    @scoped
    def finish(layer, *which):
        low, high = min(later[3 - m][0] for m in which), max(later[3 - m][1] for m in which)
        count = high - low
        rows = pl.ds(low, count)
        piece = 512
        squares, mm, ahead = 0.0, 0.0, None

        def widen(at):
            return jnp.dot(mixed[rows, :], (wo, wo_out)[layer][:, pl.ds(at, piece)], preferred_element_type=F32)

        update = widen(0)
        for at in range(0, width, piece):
            columns = pl.ds(at, piece)
            if at + piece < width:
                ahead = widen(at + piece)
            state = (x[rows, columns].astype(F32) + update).astype(BF16)
            update = ahead
            if layer == layers - 1:
                out[rows, columns] = state
                continue
            x[rows, columns] = state
            if low == 0:
                out[rows, columns] = state
            state = state.astype(F32)
            scaled = (state * gain[pl.ds(layer + 1, 1), columns]).astype(BF16)
            mm = mm + jnp.dot(scaled, w[layer + 1, columns, :], preferred_element_type=F32)
            squares = squares + sum(state[:, q : q + LANES] * state[:, q : q + LANES] for q in range(0, piece, LANES))
        if layer < layers - 1:
            gate(layer + 1, low, count, row_scale(squares), mm)
            send(layer + 1, low, high)

    @scoped
    def step(layer, m):
        transform(layer, m - 4)
        convolve(layer, m)
        if m > 0:
            foresee(layer, m - 1)
        pair(layer, m).start()

    @scoped
    def last(layer):
        mix(layer, 0)
        if layer == 0:
            transform(1, 1)
        if layer < layers - 1:
            finish(layer, 0)

    arrived("gain", ("x", 0))
    prepare(*first[0])
    project(*first[0], PIECES)
    with jax.named_scope("barrier"):

        @pl.when(has_next)
        def _():
            pl.semaphore_wait(barrier, 2)

        @pl.when(jnp.logical_not(has_next))
        def _():
            pl.semaphore_wait(barrier, 1)

    send(0, *first[0])
    for i in (1, 2, 3):
        arrived(("x", i))
        prepare(*first[i])
        project(*first[i])
        send(0, *first[i])
    arrived("fwd", "rev", "taps", "inv", "bias", "cgain", "cshift")
    for s in (3, 2, 1, 0):
        transform(0, s)
    tap_spectra(0)
    foresee(0, 3)
    tap_spectra(1)

    for layer in range(layers):
        received(layer, 0, 1)
        send_relay(layer)
        step(layer, 3)
        received(layer, 2, 3)
        step(layer, 2)
        if layer == 0:
            arrived(("wo", 0), ("wv", 1), ("wg", 1))
        paired(layer, 3)
        mix(layer, 3)
        finish(layer, 3)
        received(layer, 4, 5)
        step(layer, 1)
        if layer == layers - 1:
            received(layer, 6, 7)
            step(layer, 0)
        paired(layer, 2)
        mix(layer, 2)
        finish(layer, 2)
        if layer < layers - 1:
            received(layer, 6, 7)
            step(layer, 0)
        paired(layer, 1)
        mix(layer, 1)
        if layer == 0:
            transform(1, 3)
            transform(1, 2)
        finish(layer, 1)
        paired(layer, 0)
        last(layer)
        if layer == 0:
            transform(1, 0)
            foresee(1, 3)
            arrived(("wo", 1))

    for layer in range(layers):
        for m in range(4):
            pair(layer, m).wait_send()

        @pl.when(has_next)
        def _():
            for j in range(chunks):
                chunk(layer, j).wait_send()
            relay(layer).wait_send()


def close(result, mixed, wo, out_hbm, block, sem):
    tokens, width = result.shape
    count = mixed.shape[0]
    rest = pl.ds(count, tokens - count)
    copies = [pltpu.make_async_copy(result.at[rest], out_hbm.at[rest], sem.at[0])]
    copies[0].start()
    piece = 512
    for i, at in enumerate(range(0, width, piece)):
        columns = pl.ds(at, piece)
        update = jnp.dot(mixed[...], wo[:, columns], preferred_element_type=F32)
        block[:, columns] = (result[pl.ds(0, count), columns].astype(F32) + update).astype(BF16)
        copies.append(
            pltpu.make_async_copy(block.at[:, columns], out_hbm.at[pl.ds(0, count), columns], sem.at[1 + i])
        )
        copies[-1].start()
    for copy in copies:
        copy.wait()


def per_device(
    devices,
    stream,
    norm_gain,
    value_weight,
    gate_weight,
    conv_taps,
    conv_bias,
    channel_gain,
    channel_shift,
    out_weight,
):
    tokens, width = stream.shape
    layers, span, half = conv_taps.shape
    padded = -(-tokens // BLOCK) * BLOCK
    forward, reverse, inverse = (jnp.asarray(m) for m in spectra())
    dma = pltpu.SemaphoreType.DMA
    result, mixed, wo = pl.pallas_call(
        functools.partial(kernel, devices),
        out_shape=(
            pltpu.VMEM((tokens, width), BF16),
            pltpu.VMEM((BLOCK, 2 * half), BF16),
            pltpu.VMEM((2 * half, width), BF16),
        ),
        in_specs=[pl.BlockSpec(memory_space=pltpu.HBM)] * 12,
        out_specs=[pl.BlockSpec(memory_space=pltpu.VMEM)] * 3,
        scratch_shapes=[
            pltpu.VMEM((tokens, width), BF16),
            pltpu.VMEM((layers, width, 2 * half), BF16),
            pltpu.VMEM((2 * half, width), BF16),
            pltpu.VMEM((layers, span, half), BF16),
            pltpu.VMEM((layers, width), F32),
            pltpu.VMEM((layers, half), F32),
            pltpu.VMEM((layers, 2 * half), F32),
            pltpu.VMEM((layers, 2 * half), F32),
            pltpu.VMEM(forward.shape, BF16),
            pltpu.VMEM(reverse.shape, BF16),
            pltpu.VMEM(inverse.shape, BF16),
            pltpu.VMEM((2 * BLOCK, width), BF16),
            pltpu.VMEM((layers, padded, half), BF16),
            pltpu.VMEM((layers, span, half), BF16),
            pltpu.VMEM((layers, 8, 2 * BLOCK, half), F32),
            pltpu.VMEM((layers, 5, 2 * BLOCK, half), F32),
            pltpu.VMEM((4, 2 * BLOCK, half), F32),
            pltpu.VMEM((4 * BLOCK, half), BF16),
            pltpu.VMEM((2, 2 * BLOCK, half), F32),
            pltpu.VMEM((BLOCK, LANES), F32),
            pltpu.VMEM((layers, 2, tokens, half), BF16),
            pltpu.VMEM((tokens, 2 * half), BF16),
            dma((32,)),
            dma((layers, tokens // CHUNK)),
            dma((layers, tokens // CHUNK)),
            dma((layers,)),
            dma((layers,)),
            dma((layers, 4)),
            dma((layers, 4)),
        ],
        compiler_params=pltpu.CompilerParams(
            collective_id=0, has_side_effects=True, vmem_limit_bytes=59 * 1024 * 1024
        ),
        name="stacked_conv",
    )(
        stream, norm_gain, value_weight, gate_weight, conv_taps, conv_bias, channel_gain, channel_shift, out_weight,
        forward, reverse, inverse,
    )
    return pl.pallas_call(
        close,
        out_shape=jax.ShapeDtypeStruct((tokens, width), BF16),
        in_specs=[pl.BlockSpec(memory_space=pltpu.VMEM)] * 3,
        out_specs=pl.BlockSpec(memory_space=pl.ANY),
        scratch_shapes=[pltpu.VMEM((BLOCK, width), BF16), dma((5,))],
        compiler_params=pltpu.CompilerParams(vmem_limit_bytes=16 * 1024 * 1024),
        name="close",
    )(result, mixed, wo)


def solution(mesh):
    return jax.shard_map(
        functools.partial(per_device, mesh.shape["sp"]),
        mesh=mesh,
        in_specs=(
            P("sp", None),
            P(),
            P(None, None, "tp"),
            P(None, None, "tp"),
            P(None, None, "tp"),
            P(None, "tp"),
            P(),
            P(),
            P(),
        ),
        out_specs=P("sp", None),
        check_vma=False,
    )
```
